512 devices in a mesh: sp: 64 (over z, y), dp: 8 (over x, core).
Axes of the slice: x: 4, y: 8, z: 8, core: 2. Of those that a mesh axis runs over, the one named last changes fastest.
Arguments:
- glu_value: bfloat16 [8, 32768, 512], P('dp', 'sp'), may hold values from -6 to 6
- glu_gate: bfloat16 [8, 32768, 512], P('dp', 'sp'), may hold values from -8 to 8
- cotangent: bfloat16 [8, 32768, 2048], P('dp', 'sp'), may hold values from -8 to 8
- conv_weight: float32 [31, 512], replicated, may hold values from -1 to 1
- norm_gain: float32 [512], replicated, may hold values from 0.1 to 1.9
- norm_shift: float32 [512], replicated, may hold values from -3 to 3
- out_weight: bfloat16 [2048, 512], P('dp'), may hold values from -0.25 to 0.25
Outputs:
- grad_value: bfloat16 [8, 32768, 512], P('dp', 'sp')
- grad_gate: bfloat16 [8, 32768, 512], P('dp', 'sp')
- grad_out_weight: float32 [2048, 512], P('dp')
- grad_conv: float32 [31, 512], replicated
- grad_gain: float32 [512], replicated
- grad_shift: float32 [512], replicated
The draws below stay inside these ranges and needn't reach their ends.
All inputs are finite; a program needn't handle non-finite values.
Results may differ from the reference program's by a relative error of at most 0.003.
Values may be sent and summed in bfloat16 or wider, within the bound.
No kernel may reach another device: no remote copies, remote signals or barrier semaphores. Data moves between devices by JAX's collectives and lax.ppermute only.
A program may use at most 64 MiB of HBM per device.

```python
import math
import jax
import jax.numpy as jnp
from jax import lax

D = 2048
C = 512
SPAN = 31
SEQS = 8
LENGTH = 32768
TOKENS = 262144


def strengthened(drawn, stream_key, source, target, shards_of, factor):
    owner, partner = [(jnp.arange(drawn.shape[dim]) // (drawn.shape[dim] // shards_of)).reshape([-1 if axis == dim else 1 for axis in range(drawn.ndim)]) for dim in (source, target)]
    chosen = jax.random.permutation(stream_key, shards_of)[partner]
    strong = (owner == chosen) | (owner == (partner + shards_of // 2) % shards_of)
    return jnp.where(strong, factor * drawn, drawn)


def steps_of(stream_key, extent, split, low, high):
    def one(position, shards_of):
        heights = jax.random.uniform(jax.random.fold_in(jax.random.fold_in(stream_key, 6), position), (shards_of,), jnp.float32, low / len(split), high / len(split))
        return jnp.repeat(jnp.exp(heights), extent[position] // shards_of).reshape((-1,) + (1,) * (len(extent) - position - 1))

    gain = one(*split[0])
    for cut in split[1:]:
        gain = gain * one(*cut)
    return gain


def scatter_about(stream_key, dims, width, limit, cuts=(), held_as=jnp.bfloat16):
    drawn = width * jax.random.normal(stream_key, dims, jnp.float32)
    if cuts:
        drawn = drawn * steps_of(stream_key, dims, cuts, -0.22, 0.18)
    return jnp.clip(drawn, -limit, limit).astype(held_as)


def bell_draw_with(own_key, dims, width, bound, split, heavy, kind=jnp.bfloat16):
    values = width * jax.random.normal(own_key, dims, jnp.float32)
    if split:
        values = values * steps_of(own_key, dims, split, -0.22, 0.18)
    return jnp.clip(strengthened(values, jax.random.fold_in(own_key, 3), *heavy), -bound, bound).astype(kind)


def setup_inputs(seed: int = 0) -> dict:
    keys = jax.random.split(jax.random.key(seed), 8)
    return {
        "glu_value": scatter_about(keys[0], (SEQS, LENGTH, C), 1.0, 6.0, ((0, 8), (1, 64))),
        "glu_gate": scatter_about(keys[1], (SEQS, LENGTH, C), 1.5, 8.0, ((0, 8), (1, 64))),
        "cotangent": bell_draw_with(keys[2], (SEQS, LENGTH, D), 1.0, 8.0, ((0, 8), (1, 64)), (1, 2, 64, 4.0)),
        "conv_weight": scatter_about(keys[3], (SPAN, C), SPAN ** -0.5, 1.0, (), jnp.float32),
        "norm_gain": jnp.clip(1.0 + 0.18 * jax.random.normal(keys[4], (C,), jnp.float32), 0.1, 1.9),
        "norm_shift": scatter_about(keys[5], (C,), 0.5, 3.0, (), jnp.float32),
        "out_weight": scatter_about(keys[6], (D, C), C ** -0.5, 0.25, ((0, 8),)),
    }


epsilon = 1e-06

def sequence_grads(value_rows, gate_rows, cotan_rows, conv_weight, norm_gain, norm_shift, out_weight):
    length = value_rows.shape[0]
    channels = value_rows.shape[1]
    tap_count = conv_weight.shape[0]
    value_full = value_rows.astype(jnp.float32)
    gate_full = gate_rows.astype(jnp.float32)
    sigmoid_gate = jax.nn.sigmoid(gate_full)
    gated = value_full * sigmoid_gate
    padded = jnp.concatenate([jnp.zeros((tap_count - 1, channels), jnp.float32), gated], axis=0)
    conv_rows = jnp.zeros((length, channels), jnp.float32)
    for offset in range(tap_count):
        conv_rows = conv_rows + conv_weight[offset] * padded[offset:offset + length]
    centred = conv_rows - lax.optimization_barrier(jnp.mean(conv_rows, axis=-1, keepdims=True))
    inv_std = lax.rsqrt(lax.optimization_barrier(jnp.mean(centred * centred, axis=-1, keepdims=True)) + epsilon)
    normed = centred * inv_std
    pre_act = normed * norm_gain + norm_shift
    sigmoid_pre = jax.nn.sigmoid(pre_act)
    act_rows = (pre_act * sigmoid_pre).astype(jnp.bfloat16)
    grad_act = jnp.dot(cotan_rows, out_weight, preferred_element_type=jnp.float32)
    grad_pre = grad_act * sigmoid_pre * (1.0 + pre_act * (1.0 - sigmoid_pre))
    grad_normed = grad_pre * norm_gain
    grad_conv_rows = inv_std * (grad_normed - lax.optimization_barrier(jnp.mean(grad_normed, axis=-1, keepdims=True)) - normed * lax.optimization_barrier(jnp.mean(grad_normed * normed, axis=-1, keepdims=True)))
    padded_grad = jnp.concatenate([grad_conv_rows, jnp.zeros((tap_count - 1, channels), jnp.float32)], axis=0)
    grad_gated = jnp.zeros((length, channels), jnp.float32)
    for offset in range(tap_count):
        start = tap_count - 1 - offset
        grad_gated = grad_gated + conv_weight[offset] * padded_grad[start:start + length]
    grad_taps = jnp.stack([lax.optimization_barrier(jnp.sum(grad_conv_rows * padded[offset:offset + length], axis=0)) for offset in range(tap_count)], axis=0)
    grad_value = (grad_gated * sigmoid_gate).astype(jnp.bfloat16)
    grad_gate = (grad_gated * value_full * sigmoid_gate * (1.0 - sigmoid_gate)).astype(jnp.bfloat16)
    grad_weight = jnp.dot(cotan_rows.T, act_rows, preferred_element_type=jnp.float32)
    return (grad_value, grad_gate, grad_weight, grad_taps, lax.optimization_barrier(jnp.sum(grad_pre * normed, axis=0)), lax.optimization_barrier(jnp.sum(grad_pre, axis=0)))

def reference(glu_value, glu_gate, cotangent, conv_weight, norm_gain, norm_shift, out_weight):

    def one_sequence(items):
        return sequence_grads(items[0], items[1], items[2], conv_weight, norm_gain, norm_shift, out_weight)
    results = lax.map(one_sequence, (glu_value, glu_gate, cotangent))
    scale = 1.0 / math.sqrt(TOKENS)
    grad_out_weight = lax.optimization_barrier(jnp.sum(results[2], axis=0)) * scale
    grad_conv = lax.optimization_barrier(jnp.sum(results[3], axis=0)) * scale
    grad_gain = lax.optimization_barrier(jnp.sum(results[4], axis=0)) * scale
    grad_shift = lax.optimization_barrier(jnp.sum(results[5], axis=0)) * scale
    return (results[0], results[1], grad_out_weight, grad_conv, grad_gain, grad_shift)
```

```python
import functools
import math

import jax
import jax.numpy as jnp
from jax import lax
from jax.experimental import pallas as pl
from jax.experimental.pallas import tpu as pltpu
from jax.sharding import Mesh
from jax.sharding import PartitionSpec as P

SP = ("sp_0", "sp_1")
DP = ("dp_0", "dp_1")

epsilon = 1e-06

LANES = 128
HALO = 32
BF16 = jnp.bfloat16
F32 = jnp.float32
VMEM = pl.BlockSpec(memory_space=pltpu.VMEM)
SMEM = pl.BlockSpec(memory_space=pltpu.SMEM)
HBM = pl.BlockSpec(memory_space=pltpu.HBM)


def params(mib=16):
    return pltpu.CompilerParams(vmem_limit_bytes=mib * 1024 * 1024)


def cost(us):
    return pl.CostEstimate(flops=int(us * 5.0e8), bytes_accessed=1 << 20, transcendentals=0)


def sigmoid(x):
    return 0.5 * jnp.tanh(0.5 * x) + 0.5


def forward_kernel(
    taps_ref, gain_ref, shift_ref, halo_hbm, value_hbm, gate_hbm,
    act_hbm, normed_hbm, inv_hbm, slope_hbm, gated_hbm,
    halo_ref, value_ref, gate_ref, act_ref, normed_ref, inv_ref, slope_ref, gated_ref,
    in_sems, out_sems,
):
    length, channels = value_ref.shape
    blocks = channels // LANES
    tap_count = taps_ref.shape[0]
    loads = [
        pltpu.make_async_copy(halo_hbm, halo_ref, in_sems.at[0]),
        pltpu.make_async_copy(value_hbm, value_ref, in_sems.at[1]),
        pltpu.make_async_copy(gate_hbm, gate_ref, in_sems.at[2]),
    ]
    for load in loads:
        load.start()
    for load in loads:
        load.wait()
    for b in range(blocks):
        lanes = slice(b * LANES, (b + 1) * LANES)
        gated_ref[b, 0:HALO, :] = halo_ref[0:HALO, lanes].astype(F32) * sigmoid(
            halo_ref[HALO : 2 * HALO, lanes].astype(F32)
        )

        def gating(i, carry, b=b, lanes=lanes):
            rows = pl.ds(pl.multiple_of(i * 64, 64), 64)
            gated_ref[b, pl.ds(pl.multiple_of(HALO + i * 64, 32), 64), :] = value_ref[
                rows, lanes
            ].astype(F32) * sigmoid(gate_ref[rows, lanes].astype(F32))
            return carry

        lax.fori_loop(0, length // 64, gating, 0)

        def conv(i, carry, b=b, lanes=lanes):
            start = pl.multiple_of(i * 64, 64)
            total = jnp.zeros((64, LANES), F32)
            for j in range(tap_count):
                total = total + taps_ref[j : j + 1, lanes] * gated_ref[
                    b, pl.ds(start + (HALO - tap_count + 1 + j), 64), :
                ]
            normed_ref[b, pl.ds(start, 64), :] = total
            return carry

        lax.fori_loop(0, length // 64, conv, 0)
    stores = [pltpu.make_async_copy(gated_ref, gated_hbm, out_sems.at[0])]
    stores[0].start()

    def norm(i, carry):
        rows = pl.ds(pl.multiple_of(i * 64, 64), 64)
        parts = [normed_ref[b, rows, :] for b in range(blocks)]
        mean = jnp.sum(sum(parts), axis=-1, keepdims=True) / channels
        centred = [p - mean for p in parts]
        var = jnp.sum(sum(p * p for p in centred), axis=-1, keepdims=True) / channels
        inv = lax.rsqrt(var + epsilon)
        inv_ref[rows, :] = jnp.broadcast_to(inv, (64, LANES))
        for b in range(blocks):
            lanes = slice(b * LANES, (b + 1) * LANES)
            normed = centred[b] * inv
            normed_ref[b, rows, :] = normed
            pre = normed * gain_ref[:, lanes] + shift_ref[:, lanes]
            sig = sigmoid(pre)
            act = pre * sig
            act_ref[rows, lanes] = act.astype(BF16)
            slope_ref[b, rows, :] = sig + act * (1.0 - sig)
        return carry

    lax.fori_loop(0, length // 64, norm, 0)
    for n, pair in enumerate(
        (
            (act_ref, act_hbm), (normed_ref, normed_hbm), (inv_ref, inv_hbm),
            (slope_ref, slope_hbm),
        )
    ):
        store = pltpu.make_async_copy(*pair, out_sems.at[1 + n])
        store.start()
        stores.append(store)
    for store in stores:
        store.wait()


def weight_kernel(
    where_ref, act_hbm, other_act_hbm, cotan_hbm, other_cotan_hbm,
    sent_hbm, kept_hbm,
    act_ref, other_act_ref, cotan_ref, other_cotan_ref, sent_ref, kept_ref, in_sems, out_sems,
):
    wide = sent_ref.shape[1]
    group, me = where_ref[0], where_ref[1]
    loads = [
        pltpu.make_async_copy(act_hbm, act_ref, in_sems.at[0]),
        pltpu.make_async_copy(other_act_hbm, other_act_ref, in_sems.at[1]),
    ]
    for x in range(4):
        columns = pl.ds(pl.multiple_of((2 * x + me) * wide, wide), wide)
        loads.append(
            pltpu.make_async_copy(
                cotan_hbm.at[:, columns], cotan_ref.at[x], in_sems.at[2 + 2 * x]
            )
        )
        loads.append(
            pltpu.make_async_copy(
                other_cotan_hbm.at[:, columns], other_cotan_ref.at[x], in_sems.at[3 + 2 * x]
            )
        )
    for load in loads:
        load.start()
    loads[0].wait()
    loads[1].wait()
    dims = (((0,), (0,)), ((), ()))
    stores = []
    for x in range(4):
        loads[2 + 2 * x].wait()
        loads[3 + 2 * x].wait()
        term = lax.dot_general(
            cotan_ref[x], act_ref[...], dims, preferred_element_type=F32
        ) + lax.dot_general(
            other_cotan_ref[x], other_act_ref[...], dims, preferred_element_type=F32
        )
        sent_ref[x] = term.astype(BF16)

        @pl.when(group == x)
        def _():
            kept_ref[...] = term

        store = pltpu.make_async_copy(sent_ref.at[x], sent_hbm.at[x], out_sems.at[x])
        store.start()
        stores.append(store)
    store = pltpu.make_async_copy(kept_ref, kept_hbm, out_sems.at[4])
    store.start()
    stores.append(store)
    for store in stores:
        store.wait()


def backward_kernel(
    where_ref, gain_ref, normed_hbm, inv_hbm, slope_hbm, gated_hbm, own_hbm, other_hbm, cotan_hbm,
    grad_hbm, head_ref, small_ref,
    normed_ref, inv_ref, slope_ref, gated_ref, own_ref, other_ref, cotan_ref, grad_ref,
    in_sems, out_sem,
):
    length = inv_ref.shape[0]
    blocks = normed_ref.shape[0]
    channels = blocks * LANES
    me = where_ref[1]
    wide = own_ref.shape[1]
    tap_count = 31
    step = 128
    loads = []
    for n, pair in enumerate(
        (
            (own_hbm, own_ref), (cotan_hbm, cotan_ref), (other_hbm, other_ref),
            (normed_hbm, normed_ref), (slope_hbm, slope_ref), (inv_hbm, inv_ref),
            (gated_hbm, gated_ref),
        )
    ):
        load = pltpu.make_async_copy(*pair, in_sems.at[n])
        load.start()
        loads.append(load)
    for load in loads[:3]:
        load.wait()

    def rows_of(i, carry):
        rows = pl.ds(pl.multiple_of(i * step, step), step)
        total = jnp.zeros((step, channels), F32)
        for x in range(4):
            own = pl.ds(pl.multiple_of((2 * x + me) * wide, wide), wide)
            other = pl.ds(pl.multiple_of((2 * x + 1 - me) * wide, wide), wide)
            total = total + jnp.dot(
                cotan_ref[rows, own], own_ref[x], preferred_element_type=F32
            )
            total = total + jnp.dot(
                cotan_ref[rows, other], other_ref[x], preferred_element_type=F32
            )
        for b in range(blocks):
            grad_ref[b, rows, :] = total[:, b * LANES : (b + 1) * LANES]
        return carry

    lax.fori_loop(0, length // step, rows_of, 0)
    for load in loads[3:6]:
        load.wait()

    def point(i, carry):
        rows = pl.ds(pl.multiple_of(i * 32, 32), 32)
        inv = inv_ref[rows, :]
        grads = []
        normeds = []
        gains = []
        shifts = []
        for b in range(blocks):
            lanes = slice(b * LANES, (b + 1) * LANES)
            normed = normed_ref[b, rows, :]
            grad_pre = grad_ref[b, rows, :] * slope_ref[b, rows, :]
            gains.append(carry[b] + jnp.sum((grad_pre * normed).reshape(4, 8, LANES), axis=0))
            shifts.append(carry[blocks + b] + jnp.sum(grad_pre.reshape(4, 8, LANES), axis=0))
            grads.append(grad_pre * gain_ref[:, lanes])
            normeds.append(normed)
        first = jnp.sum(sum(grads), axis=-1, keepdims=True) / channels
        second = (
            jnp.sum(sum(g * n for g, n in zip(grads, normeds)), axis=-1, keepdims=True) / channels
        )
        for b in range(blocks):
            grad_ref[b, rows, :] = inv * (grads[b] - first - normeds[b] * second)
        return tuple(gains + shifts)

    zero = jnp.zeros((8, LANES), F32)
    sums = lax.fori_loop(0, length // 32, point, (zero,) * (2 * blocks))
    store = pltpu.make_async_copy(grad_ref, grad_hbm, out_sem)
    store.start()
    loads[6].wait()
    for b in range(blocks):
        head_ref[b] = grad_ref[b, 0:HALO, :]
        small_ref[b] = jnp.zeros(small_ref.shape[1:], F32)
        small_ref[b, tap_count : tap_count + 1, :] = jnp.sum(sums[b], axis=0, keepdims=True)
        small_ref[b, tap_count + 1 : tap_count + 2, :] = jnp.sum(
            sums[blocks + b], axis=0, keepdims=True
        )

        def taps(i, carry, b=b):
            start = pl.multiple_of(i * 8, 8)
            grad = grad_ref[b, pl.ds(start, 8), :]
            return tuple(
                carry[j]
                + grad * gated_ref[b, pl.ds(start + (HALO - tap_count + 1 + j), 8), :]
                for j in range(tap_count)
            )

        parts = lax.fori_loop(0, length // 8, taps, (zero,) * tap_count, unroll=2)
        for j in range(tap_count):
            small_ref[b, j : j + 1, :] = jnp.sum(parts[j], axis=0, keepdims=True)
    store.wait()


def gated_kernel(
    later_ref, taps_ref, grad_hbm, value_hbm, gate_hbm, out_value_ref, out_gate_ref,
    ext_ref, value_ref, gate_ref, sems,
):
    length, channels = value_ref.shape
    blocks = channels // LANES
    tap_count = taps_ref.shape[0]
    loads = []
    for b in range(blocks):
        loads.append(
            pltpu.make_async_copy(grad_hbm.at[b], ext_ref.at[b, pl.ds(0, length)], sems.at[b])
        )
    loads.append(pltpu.make_async_copy(value_hbm, value_ref, sems.at[blocks]))
    loads.append(pltpu.make_async_copy(gate_hbm, gate_ref, sems.at[blocks + 1]))
    for load in loads:
        load.start()
    for b in range(blocks):
        ext_ref[b, length : length + HALO, :] = later_ref[b]
    for load in loads:
        load.wait()
    for b in range(blocks):
        lanes = slice(b * LANES, (b + 1) * LANES)

        def conv(i, carry, b=b, lanes=lanes):
            start = pl.multiple_of(i * 64, 64)
            rows = pl.ds(start, 64)
            total = jnp.zeros((64, LANES), F32)
            for j in range(tap_count):
                total = total + taps_ref[j : j + 1, lanes] * ext_ref[
                    b, pl.ds(start + (tap_count - 1 - j), 64), :
                ]
            sig = sigmoid(gate_ref[rows, lanes].astype(F32))
            part = total * sig
            out_value_ref[rows, lanes] = part.astype(BF16)
            out_gate_ref[rows, lanes] = (
                part * value_ref[rows, lanes].astype(F32) * (1.0 - sig)
            ).astype(BF16)
            return carry

        lax.fori_loop(0, length // 64, conv, 0)


def pack_kernel(where_ref, parts_ref, kept_ref, small_ref, out_ref):
    count = out_ref.shape[0]
    blocks, small_rows, _ = small_ref.shape
    halves = small_rows // 4
    group = where_ref[0]
    weights = [jnp.where(group == x, 0.0, 1.0) for x in range(4)]
    for i in range(count // 4):
        rows = slice(16 * i, 16 * i + 16)
        tiles = []
        for b in range(blocks):
            lanes = slice(b * LANES, (b + 1) * LANES)
            tiles.append(
                kept_ref[rows, lanes]
                + sum(parts_ref[x, rows, lanes].astype(F32) * weights[x] for x in range(4))
            )
        for k in range(2):
            for h in range(2):
                m = 4 * i + 2 * k + h
                pieces = [tiles[2 * h + t][8 * k : 8 * k + 8] for t in range(2)]
                if m < blocks * halves:
                    b, g = m // halves, m % halves
                    tile = small_ref[b, 4 * g : 4 * g + 4, :]
                    high = tile.astype(BF16).astype(F32)
                    pieces += [high, tile - high]
                else:
                    pieces.append(jnp.zeros((8, LANES), F32))
                out_ref[m] = jnp.concatenate(pieces, axis=0).astype(BF16)


def total_kernel(scale, parts_ref, rows_ref, tiles_ref):
    def add(i, carry):
        return carry + parts_ref[i].astype(F32)

    total = lax.fori_loop(
        0, parts_ref.shape[0], add, jnp.zeros(parts_ref.shape[1:], F32), unroll=8
    ) * scale
    rows_ref[...] = total[0:16]
    tile = jnp.concatenate([total[16:20] + total[20:24], jnp.zeros((4, LANES), F32)], axis=0)
    for i in range(tiles_ref.shape[0]):
        tiles_ref[i] = tile


def spread_kernel(rows_ref, tiles_ref, out_ref):
    tile = sum(tiles_ref[i] for i in range(tiles_ref.shape[0]))[0:4]
    high = tile.astype(BF16).astype(F32)
    both = jnp.concatenate([rows_ref[...], high, tile - high], axis=0).astype(BF16)

    def put(i, carry):
        out_ref[i] = both
        return carry

    lax.fori_loop(0, out_ref.shape[0], put, 0, unroll=8)


def unpack_kernel(parts_ref, weight_ref, taps_ref, gain_ref, shift_ref, small_ref):
    count = parts_ref.shape[0]
    small_rows = small_ref.shape[0]
    tap_count = taps_ref.shape[0]
    blocks = small_ref.shape[1] // LANES
    halves = small_rows // 4
    for m in range(count):
        i, h = m // 2, m % 2
        part = parts_ref[m].astype(F32)
        for t in range(2):
            weight_ref[8 * i : 8 * i + 8, (2 * h + t) * LANES : (2 * h + t + 1) * LANES] = part[
                8 * t : 8 * t + 8
            ]
        if m < blocks * halves:
            b, g = m // halves, m % halves
            small_ref[4 * g : 4 * g + 4, b * LANES : (b + 1) * LANES] = part[16:20] + part[20:24]
    taps_ref[...] = small_ref[0:tap_count, :]
    gain_ref[...] = small_ref[tap_count : tap_count + 1, :]
    shift_ref[...] = small_ref[tap_count + 1 : tap_count + 2, :]


def from_behind(value, axis, by):
    count = lax.axis_size(axis)
    pairs = [(i, i + by) for i in range(count) if 0 <= i + by < count]
    return lax.ppermute(value, axis, pairs)


def swapped(value):
    return lax.ppermute(value, "dp_1", [(0, 1), (1, 0)])


def exchanged(value, axes):
    return lax.all_to_all(value, axes, 0, 0, tiled=True)


def per_device(glu_value, glu_gate, cotangent, conv_weight, norm_gain, norm_shift, out_weight):
    value_rows = glu_value[0]
    gate_rows = glu_gate[0]
    cotan_rows = cotangent[0]
    length, channels = value_rows.shape
    blocks = channels // LANES
    features = cotan_rows.shape[1]
    wide = out_weight.shape[0]
    tap_count = conv_weight.shape[0]
    count_sp = lax.axis_size(SP)
    count_dp = lax.axis_size(DP)
    scale = 1.0 / math.sqrt(length * count_sp * count_dp)
    where = jnp.stack([lax.axis_index("dp_0"), lax.axis_index("dp_1")]).astype(jnp.int32)
    gain = norm_gain.reshape(1, channels)
    shift = norm_shift.reshape(1, channels)
    shaped = jax.ShapeDtypeStruct

    halo = jnp.concatenate([value_rows[length - HALO :], gate_rows[length - HALO :]], axis=0)
    halo = from_behind(halo, SP, 1)
    other_cotan = swapped(cotan_rows)
    own_weight = exchanged(jnp.broadcast_to(out_weight[None], (4, *out_weight.shape)), "dp_0")

    act, normed, inv, slope, gated = pl.pallas_call(
        forward_kernel,
        out_shape=(
            shaped((length, channels), BF16),
            shaped((blocks, length, LANES), F32),
            shaped((length, LANES), F32),
            shaped((blocks, length, LANES), F32),
            shaped((blocks, length + HALO, LANES), F32),
        ),
        in_specs=[VMEM] * 3 + [HBM] * 3,
        out_specs=(HBM,) * 5,
        scratch_shapes=[
            pltpu.VMEM((2 * HALO, channels), BF16),
            pltpu.VMEM((length, channels), BF16),
            pltpu.VMEM((length, channels), BF16),
            pltpu.VMEM((length, channels), BF16),
            pltpu.VMEM((blocks, length, LANES), F32),
            pltpu.VMEM((length, LANES), F32),
            pltpu.VMEM((blocks, length, LANES), F32),
            pltpu.VMEM((blocks, length + HALO, LANES), F32),
            pltpu.SemaphoreType.DMA((3,)),
            pltpu.SemaphoreType.DMA((5,)),
        ],
        compiler_params=params(63),
        cost_estimate=cost(6),
        name="module_forward",
    )(conv_weight, gain, shift, halo, value_rows, gate_rows)
    other_act = swapped(act)
    own_weight, act = lax.optimization_barrier((own_weight, act))
    other_weight = swapped(own_weight)
    sent, kept = pl.pallas_call(
        weight_kernel,
        out_shape=(shaped((4, wide, channels), BF16), shaped((wide, channels), F32)),
        in_specs=[SMEM] + [HBM] * 4,
        out_specs=(HBM,) * 2,
        scratch_shapes=[
            pltpu.VMEM((length, channels), BF16),
            pltpu.VMEM((length, channels), BF16),
            pltpu.VMEM((4, length, wide), BF16),
            pltpu.VMEM((4, length, wide), BF16),
            pltpu.VMEM((4, wide, channels), BF16),
            pltpu.VMEM((wide, channels), F32),
            pltpu.SemaphoreType.DMA((10,)),
            pltpu.SemaphoreType.DMA((5,)),
        ],
        compiler_params=params(63),
        cost_estimate=cost(3),
        name="weight_term",
    )(where, act, other_act, cotan_rows, other_cotan)
    arrived = exchanged(sent, "dp_0")

    small_rows = -(-(tap_count + 2) // 8) * 8
    grad, head, small = pl.pallas_call(
        backward_kernel,
        out_shape=(
            shaped((blocks, length, LANES), F32),
            shaped((blocks, HALO, LANES), F32),
            shaped((blocks, small_rows, LANES), F32),
        ),
        in_specs=[SMEM, VMEM] + [HBM] * 7,
        out_specs=(HBM, VMEM, VMEM),
        scratch_shapes=[
            pltpu.VMEM((blocks, length, LANES), F32),
            pltpu.VMEM((length, LANES), F32),
            pltpu.VMEM((blocks, length, LANES), F32),
            pltpu.VMEM((blocks, length + HALO, LANES), F32),
            pltpu.VMEM((4, wide, channels), BF16),
            pltpu.VMEM((4, wide, channels), BF16),
            pltpu.VMEM((length, features), BF16),
            pltpu.VMEM((blocks, length, LANES), F32),
            pltpu.SemaphoreType.DMA((7,)),
            pltpu.SemaphoreType.DMA,
        ],
        compiler_params=params(63),
        cost_estimate=cost(10),
        name="module_backward",
    )(where, gain, normed, inv, slope, gated, own_weight, other_weight, cotan_rows)
    later = from_behind(head, SP, -1)

    packed = pl.pallas_call(
        pack_kernel,
        out_shape=shaped((count_sp, 24, LANES), BF16),
        in_specs=[SMEM] + [VMEM] * 3,
        out_specs=VMEM,
        compiler_params=params(8),
        cost_estimate=cost(1),
        name="pack",
    )(where, arrived, kept, small)
    packed, later = lax.optimization_barrier((packed, later))
    grad_value, grad_gate = pl.pallas_call(
        gated_kernel,
        out_shape=(shaped((length, channels), BF16), shaped((length, channels), BF16)),
        in_specs=[VMEM] * 2 + [HBM] * 3,
        out_specs=(VMEM,) * 2,
        scratch_shapes=[
            pltpu.VMEM((blocks, length + HALO, LANES), F32),
            pltpu.VMEM((length, channels), BF16),
            pltpu.VMEM((length, channels), BF16),
            pltpu.SemaphoreType.DMA((blocks + 2,)),
        ],
        compiler_params=params(63),
        cost_estimate=cost(6),
        name="gated_backward",
    )(later, conv_weight, grad, value_rows, gate_rows)

    terms = exchanged(packed, SP)
    rows, tiles = pl.pallas_call(
        functools.partial(total_kernel, scale),
        out_shape=(shaped((16, LANES), F32), shaped((count_dp, 8, LANES), F32)),
        in_specs=[VMEM],
        out_specs=(VMEM,) * 2,
        compiler_params=params(4),
        cost_estimate=cost(1),
        name="total",
    )(terms)
    tiles = exchanged(tiles, DP)
    totals = pl.pallas_call(
        spread_kernel,
        out_shape=shaped((count_sp, 24, LANES), BF16),
        in_specs=[VMEM] * 2,
        out_specs=VMEM,
        compiler_params=params(4),
        cost_estimate=cost(1),
        name="spread",
    )(rows, tiles)
    whole = exchanged(totals, SP)
    grad_out_weight, grad_conv, grad_gain, grad_shift = pl.pallas_call(
        unpack_kernel,
        out_shape=(
            shaped((wide, channels), F32),
            shaped((tap_count, channels), F32),
            shaped((1, channels), F32),
            shaped((1, channels), F32),
        ),
        in_specs=[VMEM],
        out_specs=(VMEM,) * 4,
        scratch_shapes=[pltpu.VMEM((small_rows, channels), F32)],
        compiler_params=params(8),
        cost_estimate=cost(1),
        name="unpack",
    )(whole)
    return (
        grad_value[None],
        grad_gate[None],
        grad_out_weight,
        grad_conv,
        grad_gain.reshape(channels),
        grad_shift.reshape(channels),
    )


def solution(mesh):
    split = Mesh(mesh.devices.reshape(8, 8, 4, 2), ("sp_0", "sp_1", "dp_0", "dp_1"))
    return jax.shard_map(
        per_device,
        mesh=split,
        in_specs=(P(DP, SP, None), P(DP, SP, None), P(DP, SP, None), P(), P(), P(), P(DP, None)),
        out_specs=(P(DP, SP, None), P(DP, SP, None), P(DP, None), P(), P(), P()),
        check_vma=False,
    )
```

```python
import functools
import math

import jax
import jax.numpy as jnp
from jax import lax
from jax.experimental import pallas as pl
from jax.experimental.pallas import tpu as pltpu
from jax.sharding import Mesh
from jax.sharding import PartitionSpec as P


SP = ("sp_0", "sp_1")
DP = ("dp_0", "dp_1")

epsilon = 1e-06

LANES = 128
HALO = 32
BF16 = jnp.bfloat16
F32 = jnp.float32
VMEM = pl.BlockSpec(memory_space=pltpu.VMEM)
HBM = pl.BlockSpec(memory_space=pltpu.HBM)


def params(mib=16):
    return pltpu.CompilerParams(vmem_limit_bytes=mib * 1024 * 1024)


def cost(us):
    return pl.CostEstimate(flops=int(us * 5.0e8), bytes_accessed=1 << 20, transcendentals=0)


def sigmoid(x):
    return 0.5 * jnp.tanh(0.5 * x) + 0.5


def convolved(load, weights, groups):
    totals = [None] * groups
    for o in range(8 * (groups - 1) + len(weights)):
        rows = load(o)
        for q in range(groups):
            j = o - 8 * q
            if 0 <= j < len(weights):
                term = weights[j] * rows
                totals[q] = term if totals[q] is None else totals[q] + term
    return totals


def prepare_kernel(value_hbm, gate_hbm, weight_hbm, halo_ref, copies_hbm, weight_ref, sems):
    length = value_hbm.shape[0]
    tail = pl.ds(length - HALO, HALO)
    loads = [
        pltpu.make_async_copy(weight_hbm, weight_ref, sems.at[0]),
        pltpu.make_async_copy(value_hbm.at[tail], halo_ref.at[pl.ds(0, HALO)], sems.at[1]),
        pltpu.make_async_copy(gate_hbm.at[tail], halo_ref.at[pl.ds(HALO, HALO)], sems.at[2]),
    ]
    for load in loads:
        load.start()
    loads[0].wait()
    stores = [
        pltpu.make_async_copy(weight_ref, copies_hbm.at[x], sems.at[3 + x]) for x in range(4)
    ]
    for store in stores:
        store.start()
    for copy in loads[1:] + stores:
        copy.wait()


def forward_kernel(
    taps_ref, gain_ref, shift_ref, halo_ref, value_ref, gate_ref,
    act_ref, normed_hbm, inv_hbm,
    normed_ref, inv_ref, gated_ref, out_sems,
):
    length, channels = value_ref.shape
    blocks = channels // LANES
    tap_count = taps_ref.shape[0]
    step = 64
    steps = length // step

    def row_stores(i):
        rows = pl.ds(pl.multiple_of(i * step, step), step)
        return [
            pltpu.make_async_copy(inv_ref.at[rows], inv_hbm.at[rows], out_sems.at[0, i]),
            pltpu.make_async_copy(
                normed_ref.at[:, rows], normed_hbm.at[:, rows], out_sems.at[1, i]
            ),
        ]

    for b in range(blocks):
        lanes = slice(b * LANES, (b + 1) * LANES)
        gated_ref[b, 0:HALO, :] = halo_ref[0:HALO, lanes].astype(F32) * sigmoid(
            halo_ref[HALO : 2 * HALO, lanes].astype(F32)
        )

    def group(i, carry):
        start = pl.multiple_of(i * step, step)
        rows = pl.ds(start, step)
        for b in range(blocks):
            lanes = slice(b * LANES, (b + 1) * LANES)
            gated_ref[b, pl.ds(pl.multiple_of(HALO + start, 32), step), :] = value_ref[
                rows, lanes
            ].astype(F32) * sigmoid(gate_ref[rows, lanes].astype(F32))
        for b in range(blocks):
            lanes = slice(b * LANES, (b + 1) * LANES)
            totals = convolved(
                lambda o: gated_ref[b, pl.ds(start + (HALO - tap_count + 1 + o), 8), :],
                [
                    jnp.broadcast_to(taps_ref[j : j + 1, lanes], (8, LANES))
                    for j in range(tap_count)
                ],
                step // 8,
            )
            for q, total in enumerate(totals):
                normed_ref[b, pl.ds(pl.multiple_of(start + 8 * q, 8), 8), :] = total
        parts = [normed_ref[b, rows, :] for b in range(blocks)]
        mean = jnp.sum(sum(parts), axis=-1, keepdims=True) / channels
        centred = [p - mean for p in parts]
        var = jnp.sum(sum(p * p for p in centred), axis=-1, keepdims=True) / channels
        inv = lax.rsqrt(var + epsilon)
        inv_ref[rows, :] = jnp.broadcast_to(inv, (step, LANES))
        for b in range(blocks):
            lanes = slice(b * LANES, (b + 1) * LANES)
            normed = centred[b] * inv
            normed_ref[b, rows, :] = normed
            pre = normed * gain_ref[:, lanes] + shift_ref[:, lanes]
            act_ref[rows, lanes] = (pre * sigmoid(pre)).astype(BF16)
        for store in row_stores(i):
            store.start()
        return carry

    lax.fori_loop(0, steps, group, 0)
    for i in range(steps):
        for store in row_stores(i):
            store.wait()


def weight_kernel(
    act_ref, other_act_ref, cotan_ref, other_cotan_ref, sent_hbm, kept_hbm,
    sent_ref, kept_ref, out_sems,
):
    wide = sent_ref.shape[1]
    group, me = lax.axis_index("dp_0"), lax.axis_index("dp_1")
    dims = (((0,), (0,)), ((), ()))
    stores = []
    for k in range(4):
        x = lax.rem(group + k, 4)
        columns = pl.ds(pl.multiple_of((2 * x + me) * wide, wide), wide)
        term = lax.dot_general(
            cotan_ref[:, columns], act_ref[...], dims, preferred_element_type=F32
        ) + lax.dot_general(
            other_cotan_ref[:, columns], other_act_ref[...], dims, preferred_element_type=F32
        )
        sent_ref[k] = term.astype(BF16)
        if k == 0:
            kept_ref[...] = term
            stores.append(pltpu.make_async_copy(kept_ref, kept_hbm, out_sems.at[4]))
            stores[-1].start()
        stores.append(pltpu.make_async_copy(sent_ref.at[k], sent_hbm.at[x], out_sems.at[k]))
        stores[-1].start()
    for store in stores:
        store.wait()


def backward_kernel(
    gain_hbm, shift_hbm, normed_hbm, inv_hbm, halo_hbm, value_hbm, gate_hbm, own_hbm, other_ref,
    cotan_hbm,
    grad_hbm, head_ref, small_ref,
    gain_ref, shift_ref, normed_ref, inv_ref, halo_ref, value_ref, gate_ref, own_ref,
    cotan_ref, grad_ref, gated_ref, cotan_sems, in_sems, out_sem,
):
    length = inv_ref.shape[0]
    blocks = normed_ref.shape[0]
    channels = blocks * LANES
    me = lax.axis_index("dp_1")
    wide = own_ref.shape[1]
    tap_count = 31
    step = 128
    columns = [
        pltpu.make_async_copy(
            cotan_hbm.at[:, pl.ds(pl.multiple_of((2 * x + parity) * wide, wide), wide)],
            cotan_ref.at[4 * n + x],
            cotan_sems.at[4 * n + x],
        )
        for n, parity in enumerate((me, 1 - me))
        for x in range(4)
    ]
    own, *rest = [
        pltpu.make_async_copy(source, target, in_sems.at[n])
        for n, (source, target) in enumerate(
            (
                (own_hbm, own_ref), (gain_hbm, gain_ref),
                (shift_hbm, shift_ref), (normed_hbm, normed_ref), (inv_hbm, inv_ref),
                (halo_hbm, halo_ref), (value_hbm, value_ref), (gate_hbm, gate_ref),
            )
        )
    ]
    for load in (*rest[4:], own, *columns, *rest[:4]):
        load.start()

    def half(n, weight_ref):
        def rows_of(i, carry):
            rows = pl.ds(pl.multiple_of(i * step, step), step)
            total = jnp.dot(cotan_ref[4 * n, rows], weight_ref[0], preferred_element_type=F32)
            for x in range(1, 4):
                total = total + jnp.dot(
                    cotan_ref[4 * n + x, rows], weight_ref[x], preferred_element_type=F32
                )
            for b in range(blocks):
                part = total[:, b * LANES : (b + 1) * LANES]
                grad_ref[b, rows, :] = part + grad_ref[b, rows, :] if n else part
            return carry

        lax.fori_loop(0, length // step, rows_of, 0)

    for load in rest[4:]:
        load.wait()
    for b in range(blocks):
        lanes = slice(b * LANES, (b + 1) * LANES)
        gated_ref[b, 0:HALO, :] = halo_ref[0:HALO, lanes].astype(F32) * sigmoid(
            halo_ref[HALO : 2 * HALO, lanes].astype(F32)
        )

        def gating(i, carry, b=b, lanes=lanes):
            rows = pl.ds(pl.multiple_of(i * 64, 64), 64)
            gated_ref[b, pl.ds(pl.multiple_of(HALO + i * 64, 32), 64), :] = value_ref[
                rows, lanes
            ].astype(F32) * sigmoid(gate_ref[rows, lanes].astype(F32))
            return carry

        lax.fori_loop(0, length // 64, gating, 0)

    for load in (own, *columns[:4]):
        load.wait()
    half(0, own_ref)
    for load in columns[4:]:
        load.wait()
    half(1, other_ref)
    for load in rest[:4]:
        load.wait()

    def point(i, carry):
        rows = pl.ds(pl.multiple_of(i * 32, 32), 32)
        inv = inv_ref[rows, :]
        grads = []
        normeds = []
        gains = []
        shifts = []
        for b in range(blocks):
            lanes = slice(b * LANES, (b + 1) * LANES)
            normed = normed_ref[b, rows, :]
            pre = normed * gain_ref[:, lanes] + shift_ref[:, lanes]
            sig = sigmoid(pre)
            grad_pre = grad_ref[b, rows, :] * (sig + pre * sig * (1.0 - sig))
            gains.append(carry[b] + jnp.sum((grad_pre * normed).reshape(4, 8, LANES), axis=0))
            shifts.append(carry[blocks + b] + jnp.sum(grad_pre.reshape(4, 8, LANES), axis=0))
            grads.append(grad_pre * gain_ref[:, lanes])
            normeds.append(normed)
        first = jnp.sum(sum(grads), axis=-1, keepdims=True) / channels
        second = (
            jnp.sum(sum(g * n for g, n in zip(grads, normeds)), axis=-1, keepdims=True) / channels
        )
        for b in range(blocks):
            grad_ref[b, rows, :] = inv * (grads[b] - first - normeds[b] * second)
        return tuple(gains + shifts)

    zero = jnp.zeros((8, LANES), F32)
    sums = lax.fori_loop(0, length // 32, point, (zero,) * (2 * blocks))
    store = pltpu.make_async_copy(grad_ref, grad_hbm, out_sem)
    store.start()
    for b in range(blocks):
        head_ref[b] = grad_ref[b, 0:HALO, :]
        small_ref[b] = jnp.zeros(small_ref.shape[1:], F32)
        small_ref[b, tap_count : tap_count + 1, :] = jnp.sum(sums[b], axis=0, keepdims=True)
        small_ref[b, tap_count + 1 : tap_count + 2, :] = jnp.sum(
            sums[blocks + b], axis=0, keepdims=True
        )

        def taps(i, carry, b=b):
            start = pl.multiple_of(i * 32, 32)
            grads = [
                grad_ref[b, pl.ds(pl.multiple_of(start + 8 * q, 8), 8), :] for q in range(4)
            ]
            parts = list(carry)
            for o in range(24 + tap_count):
                rows = gated_ref[b, pl.ds(start + (HALO - tap_count + 1 + o), 8), :]
                for q in range(4):
                    if 0 <= o - 8 * q < tap_count:
                        parts[o - 8 * q] = parts[o - 8 * q] + grads[q] * rows
            return tuple(parts)

        parts = lax.fori_loop(0, length // 32, taps, (zero,) * tap_count)
        for j in range(tap_count):
            small_ref[b, j : j + 1, :] = jnp.sum(parts[j], axis=0, keepdims=True)
    store.wait()


def gated_kernel(
    later_ref, taps_ref, grad_hbm, value_hbm, gate_hbm, out_value_ref, out_gate_ref,
    ext_ref, value_ref, gate_ref, sems,
):
    length, channels = value_ref.shape
    blocks = channels // LANES
    tap_count = taps_ref.shape[0]
    loads = []
    for b in range(blocks):
        loads.append(
            pltpu.make_async_copy(grad_hbm.at[b], ext_ref.at[b, pl.ds(0, length)], sems.at[b])
        )
    loads.append(pltpu.make_async_copy(value_hbm, value_ref, sems.at[blocks]))
    loads.append(pltpu.make_async_copy(gate_hbm, gate_ref, sems.at[blocks + 1]))
    for load in loads:
        load.start()
    for b in range(blocks):
        ext_ref[b, length : length + HALO, :] = later_ref[b]
    for load in loads:
        load.wait()
    for b in range(blocks):
        lanes = slice(b * LANES, (b + 1) * LANES)

        def conv(i, carry, b=b, lanes=lanes):
            start = pl.multiple_of(i * 64, 64)
            rows = pl.ds(start, 64)
            totals = convolved(
                lambda o: ext_ref[b, pl.ds(start + o, 8), :],
                [
                    jnp.broadcast_to(taps_ref[j : j + 1, lanes], (8, LANES))
                    for j in reversed(range(tap_count))
                ],
                8,
            )
            total = jnp.concatenate(totals, axis=0)
            sig = sigmoid(gate_ref[rows, lanes].astype(F32))
            part = total * sig
            out_value_ref[rows, lanes] = part.astype(BF16)
            out_gate_ref[rows, lanes] = (
                part * value_ref[rows, lanes].astype(F32) * (1.0 - sig)
            ).astype(BF16)
            return carry

        lax.fori_loop(0, length // 64, conv, 0)


def pack_kernel(parts_ref, kept_ref, small_ref, out_ref):
    count = out_ref.shape[0]
    blocks, small_rows, _ = small_ref.shape
    halves = small_rows // 4
    group = lax.axis_index("dp_0")
    weights = [jnp.where(group == x, 0.0, 1.0) for x in range(4)]
    for i in range(count // 4):
        rows = slice(16 * i, 16 * i + 16)
        tiles = []
        for b in range(blocks):
            lanes = slice(b * LANES, (b + 1) * LANES)
            tiles.append(
                kept_ref[rows, lanes]
                + sum(parts_ref[x, rows, lanes].astype(F32) * weights[x] for x in range(4))
            )
        for k in range(2):
            for h in range(2):
                m = 4 * i + 2 * k + h
                pieces = [tiles[2 * h + t][8 * k : 8 * k + 8] for t in range(2)]
                if m < blocks * halves:
                    b, g = m // halves, m % halves
                    tile = small_ref[b, 4 * g : 4 * g + 4, :]
                    high = tile.astype(BF16).astype(F32)
                    pieces += [high, tile - high]
                else:
                    pieces.append(jnp.zeros((8, LANES), F32))
                out_ref[m] = jnp.concatenate(pieces, axis=0).astype(BF16)


def total_kernel(scale, parts_ref, rows_ref, tiles_ref):
    def add(i, carry):
        return carry + parts_ref[i].astype(F32)

    total = lax.fori_loop(
        0, parts_ref.shape[0], add, jnp.zeros(parts_ref.shape[1:], F32), unroll=8
    ) * scale
    rows_ref[...] = total[0:16]
    tile = jnp.concatenate([total[16:20] + total[20:24], jnp.zeros((4, LANES), F32)], axis=0)
    for i in range(tiles_ref.shape[0]):
        tiles_ref[i] = tile


def spread_kernel(rows_ref, tiles_ref, out_ref):
    tile = sum(tiles_ref[i] for i in range(tiles_ref.shape[0]))[0:4]
    high = tile.astype(BF16).astype(F32)
    both = jnp.concatenate([rows_ref[...], high, tile - high], axis=0).astype(BF16)

    def put(i, carry):
        out_ref[i] = both
        return carry

    lax.fori_loop(0, out_ref.shape[0], put, 0, unroll=8)


def unpack_kernel(parts_ref, weight_ref, taps_ref, gain_ref, shift_ref, small_ref):
    count = parts_ref.shape[0]
    small_rows = small_ref.shape[0]
    tap_count = taps_ref.shape[0]
    blocks = small_ref.shape[1] // LANES
    halves = small_rows // 4
    for m in range(count):
        i, h = m // 2, m % 2
        part = parts_ref[m].astype(F32)
        for t in range(2):
            weight_ref[8 * i : 8 * i + 8, (2 * h + t) * LANES : (2 * h + t + 1) * LANES] = part[
                8 * t : 8 * t + 8
            ]
        if m < blocks * halves:
            b, g = m // halves, m % halves
            small_ref[4 * g : 4 * g + 4, b * LANES : (b + 1) * LANES] = part[16:20] + part[20:24]
    taps_ref[...] = small_ref[0:tap_count, :]
    gain_ref[...] = small_ref[tap_count : tap_count + 1, :]
    shift_ref[...] = small_ref[tap_count + 1 : tap_count + 2, :]


def from_behind(value, axis, by):
    count = lax.axis_size(axis)
    pairs = [(i, i + by) for i in range(count) if 0 <= i + by < count]
    return lax.ppermute(value, axis, pairs)


def swapped(value):
    return lax.ppermute(value, "dp_1", [(0, 1), (1, 0)])


def in_hbm(value):
    return pltpu.with_memory_space_constraint(value, pltpu.HBM)


def exchanged(value, axes):
    return lax.all_to_all(value, axes, 0, 0, tiled=True)


def one_device(glu_value, glu_gate, cotangent, conv_weight, norm_gain, norm_shift, out_weight):
    value_rows = glu_value[0]
    gate_rows = glu_gate[0]
    cotan_rows = cotangent[0]
    length, channels = value_rows.shape
    blocks = channels // LANES
    wide = out_weight.shape[0]
    tap_count = conv_weight.shape[0]
    count_sp = lax.axis_size(SP)
    count_dp = lax.axis_size(DP)
    scale = 1.0 / math.sqrt(length * count_sp * count_dp)
    gain = norm_gain.reshape(1, channels)
    shift = norm_shift.reshape(1, channels)
    shaped = jax.ShapeDtypeStruct

    halo, copies = pl.pallas_call(
        prepare_kernel,
        out_shape=(shaped((2 * HALO, channels), BF16), shaped((4, wide, channels), BF16)),
        in_specs=[HBM] * 3,
        out_specs=(VMEM, HBM),
        scratch_shapes=[pltpu.VMEM((wide, channels), BF16), pltpu.SemaphoreType.DMA((7,))],
        compiler_params=params(62),
        cost_estimate=cost(1),
        name="prepare",
    )(value_rows, gate_rows, out_weight)
    halo = from_behind(halo, SP, 1)
    other_cotan = swapped(cotan_rows)
    own_weight = exchanged(copies, "dp_0")

    act, normed, inv = pl.pallas_call(
        forward_kernel,
        out_shape=(
            shaped((length, channels), BF16),
            pltpu.HBM((blocks, length, LANES), F32),
            pltpu.HBM((length, LANES), F32),
        ),
        in_specs=[VMEM] * 6,
        out_specs=(VMEM, HBM, HBM),
        scratch_shapes=[
            pltpu.VMEM((blocks, length, LANES), F32),
            pltpu.VMEM((length, LANES), F32),
            pltpu.VMEM((blocks, length + HALO, LANES), F32),
            pltpu.SemaphoreType.DMA((2, length // 64)),
        ],
        compiler_params=params(8),
        cost_estimate=cost(6),
        name="module_forward",
    )(conv_weight, gain, shift, halo, value_rows, gate_rows)
    other_act = swapped(act)
    sent, kept = pl.pallas_call(
        weight_kernel,
        out_shape=(pltpu.HBM((4, wide, channels), BF16), pltpu.HBM((wide, channels), F32)),
        in_specs=[VMEM] * 4,
        out_specs=(HBM,) * 2,
        scratch_shapes=[
            pltpu.VMEM((4, wide, channels), BF16),
            pltpu.VMEM((wide, channels), F32),
            pltpu.SemaphoreType.DMA((5,)),
        ],
        compiler_params=params(8),
        cost_estimate=cost(3),
        name="weight_term",
    )(act, other_act, cotan_rows, other_cotan)
    own_weight, kept = lax.optimization_barrier((own_weight, kept))
    other_weight = swapped(own_weight)
    arrived = exchanged(sent, "dp_0")

    small_rows = -(-(tap_count + 2) // 8) * 8
    grad, head, small = pl.pallas_call(
        backward_kernel,
        out_shape=(
            pltpu.HBM((blocks, length, LANES), F32),
            shaped((blocks, HALO, LANES), F32),
            shaped((blocks, small_rows, LANES), F32),
        ),
        in_specs=[HBM] * 8 + [VMEM, HBM],
        out_specs=(HBM, VMEM, VMEM),
        scratch_shapes=[
            pltpu.VMEM((1, channels), F32),
            pltpu.VMEM((1, channels), F32),
            pltpu.VMEM((blocks, length, LANES), F32),
            pltpu.VMEM((length, LANES), F32),
            pltpu.VMEM((2 * HALO, channels), BF16),
            pltpu.VMEM((length, channels), BF16),
            pltpu.VMEM((length, channels), BF16),
            pltpu.VMEM((4, wide, channels), BF16),
            pltpu.VMEM((8, length, wide), BF16),
            pltpu.VMEM((blocks, length, LANES), F32),
            pltpu.VMEM((blocks, length + HALO, LANES), F32),
            pltpu.SemaphoreType.DMA((8,)),
            pltpu.SemaphoreType.DMA((8,)),
            pltpu.SemaphoreType.DMA,
        ],
        compiler_params=params(14),
        cost_estimate=cost(10),
        name="module_backward",
    )(
        *(in_hbm(a) for a in (gain, shift, normed, inv, halo, value_rows, gate_rows)),
        in_hbm(own_weight), other_weight, in_hbm(cotan_rows),
    )
    later = from_behind(head, SP, -1)

    packed = pl.pallas_call(
        pack_kernel,
        out_shape=shaped((count_sp, 24, LANES), BF16),
        in_specs=[VMEM] * 3,
        out_specs=VMEM,
        compiler_params=params(8),
        cost_estimate=cost(1),
        name="pack",
    )(arrived, kept, small)
    grad_value, grad_gate = pl.pallas_call(
        gated_kernel,
        out_shape=(shaped((length, channels), BF16), shaped((length, channels), BF16)),
        in_specs=[VMEM] * 2 + [HBM] * 3,
        out_specs=(VMEM,) * 2,
        scratch_shapes=[
            pltpu.VMEM((blocks, length + HALO, LANES), F32),
            pltpu.VMEM((length, channels), BF16),
            pltpu.VMEM((length, channels), BF16),
            pltpu.SemaphoreType.DMA((blocks + 2,)),
        ],
        compiler_params=params(62),
        cost_estimate=cost(6),
        name="gated_backward",
    )(later, conv_weight, grad, value_rows, gate_rows)

    terms = exchanged(packed, SP)
    rows, tiles = pl.pallas_call(
        functools.partial(total_kernel, scale),
        out_shape=(shaped((16, LANES), F32), shaped((count_dp, 8, LANES), F32)),
        in_specs=[VMEM],
        out_specs=(VMEM,) * 2,
        compiler_params=params(4),
        cost_estimate=cost(1),
        name="total",
    )(terms)
    tiles = exchanged(tiles, DP)
    totals = pl.pallas_call(
        spread_kernel,
        out_shape=shaped((count_sp, 24, LANES), BF16),
        in_specs=[VMEM] * 2,
        out_specs=VMEM,
        compiler_params=params(4),
        cost_estimate=cost(1),
        name="spread",
    )(rows, tiles)
    whole = exchanged(totals, SP)
    grad_out_weight, grad_conv, grad_gain, grad_shift = pl.pallas_call(
        unpack_kernel,
        out_shape=(
            shaped((wide, channels), F32),
            shaped((tap_count, channels), F32),
            shaped((1, channels), F32),
            shaped((1, channels), F32),
        ),
        in_specs=[VMEM],
        out_specs=(VMEM,) * 4,
        scratch_shapes=[pltpu.VMEM((small_rows, channels), F32)],
        compiler_params=params(8),
        cost_estimate=cost(1),
        name="unpack",
    )(whole)
    return (
        grad_value[None],
        grad_gate[None],
        grad_out_weight,
        grad_conv,
        grad_gain.reshape(channels),
        grad_shift.reshape(channels),
    )


def solution(mesh):
    split = Mesh(mesh.devices.reshape(8, 8, 4, 2), ("sp_0", "sp_1", "dp_0", "dp_1"))
    return jax.shard_map(
        one_device,
        mesh=split,
        in_specs=(P(DP, SP, None), P(DP, SP, None), P(DP, SP, None), P(), P(), P(), P(DP, None)),
        out_specs=(P(DP, SP, None), P(DP, SP, None), P(DP, None), P(), P(), P()),
        check_vma=False,
    )
```

```python
import functools
import math

import jax
import jax.numpy as jnp
from jax import lax
from jax.experimental import pallas as pl
from jax.experimental.pallas import tpu as pltpu
from jax.sharding import Mesh
from jax.sharding import PartitionSpec as P


SP = ("sp_0", "sp_1")
DP = ("dp_0", "dp_1")

epsilon = 1e-06

LANES = 128
HALO = 32
BF16 = jnp.bfloat16
F32 = jnp.float32
VMEM = pl.BlockSpec(memory_space=pltpu.VMEM)
HBM = pl.BlockSpec(memory_space=pltpu.HBM)


def params(mib=16):
    return pltpu.CompilerParams(vmem_limit_bytes=mib * 1024 * 1024)


def cost(us):
    return pl.CostEstimate(flops=int(us * 5.0e8), bytes_accessed=1 << 20, transcendentals=0)


def sigmoid(x):
    return 0.5 * jnp.tanh(0.5 * x) + 0.5


def convolved(load, weights, groups):
    totals = [None] * groups
    for o in range(8 * (groups - 1) + len(weights)):
        rows = load(o)
        for q in range(groups):
            j = o - 8 * q
            if 0 <= j < len(weights):
                term = weights[j] * rows
                totals[q] = term if totals[q] is None else totals[q] + term
    return totals


def prepare_kernel(value_hbm, gate_hbm, weight_hbm, halo_ref, copies_hbm, weight_ref, sems):
    length = value_hbm.shape[0]
    tail = pl.ds(length - HALO, HALO)
    loads = [
        pltpu.make_async_copy(weight_hbm, weight_ref, sems.at[0]),
        pltpu.make_async_copy(value_hbm.at[tail], halo_ref.at[pl.ds(0, HALO)], sems.at[1]),
        pltpu.make_async_copy(gate_hbm.at[tail], halo_ref.at[pl.ds(HALO, HALO)], sems.at[2]),
    ]
    for load in loads:
        load.start()
    loads[0].wait()
    stores = [
        pltpu.make_async_copy(weight_ref, copies_hbm.at[x], sems.at[3 + x]) for x in range(4)
    ]
    for store in stores:
        store.start()
    for copy in loads[1:] + stores:
        copy.wait()


def forward_kernel(
    taps_ref, gain_ref, shift_ref, halo_ref, value_ref, gate_ref,
    act_ref, normed_hbm, inv_hbm,
    normed_ref, inv_ref, gated_ref, out_sems,
):
    length, channels = value_ref.shape
    blocks = channels // LANES
    tap_count = taps_ref.shape[0]
    step = 128
    steps = length // step

    def row_stores(i):
        rows = pl.ds(pl.multiple_of(i * step, step), step)
        return [
            pltpu.make_async_copy(inv_ref.at[rows], inv_hbm.at[rows], out_sems.at[0, i]),
            pltpu.make_async_copy(
                normed_ref.at[:, rows], normed_hbm.at[:, rows], out_sems.at[1, i]
            ),
        ]

    for b in range(blocks):
        lanes = slice(b * LANES, (b + 1) * LANES)
        gated_ref[b, 0:HALO, :] = halo_ref[0:HALO, lanes].astype(F32) * sigmoid(
            halo_ref[HALO : 2 * HALO, lanes].astype(F32)
        )

    def group(i, carry):
        start = pl.multiple_of(i * step, step)
        rows = pl.ds(start, step)
        for b in range(blocks):
            lanes = slice(b * LANES, (b + 1) * LANES)
            gated_ref[b, pl.ds(pl.multiple_of(HALO + start, 32), step), :] = value_ref[
                rows, lanes
            ].astype(F32) * sigmoid(gate_ref[rows, lanes].astype(F32))
        for b in range(blocks):
            lanes = slice(b * LANES, (b + 1) * LANES)
            totals = convolved(
                lambda o: gated_ref[b, pl.ds(start + (HALO - tap_count + 1 + o), 8), :],
                [
                    jnp.broadcast_to(taps_ref[j : j + 1, lanes], (8, LANES))
                    for j in range(tap_count)
                ],
                step // 8,
            )
            for q, total in enumerate(totals):
                normed_ref[b, pl.ds(pl.multiple_of(start + 8 * q, 8), 8), :] = total
        parts = [normed_ref[b, rows, :] for b in range(blocks)]
        mean = jnp.sum(sum(parts), axis=-1, keepdims=True) / channels
        centred = [p - mean for p in parts]
        var = jnp.sum(sum(p * p for p in centred), axis=-1, keepdims=True) / channels
        inv = lax.rsqrt(var + epsilon)
        inv_ref[rows, :] = jnp.broadcast_to(inv, (step, LANES))
        for b in range(blocks):
            lanes = slice(b * LANES, (b + 1) * LANES)
            normed = centred[b] * inv
            normed_ref[b, rows, :] = normed
            pre = normed * gain_ref[:, lanes] + shift_ref[:, lanes]
            act_ref[rows, lanes] = (pre * sigmoid(pre)).astype(BF16)
        for store in row_stores(i):
            store.start()
        return carry

    lax.fori_loop(0, steps, group, 0)
    for i in range(steps):
        for store in row_stores(i):
            store.wait()


def weight_kernel(
    act_ref, other_act_ref, cotan_ref, other_cotan_ref, sent_hbm, kept_hbm,
    sent_ref, kept_ref, out_sems,
):
    wide = sent_ref.shape[1]
    group, me = lax.axis_index("dp_0"), lax.axis_index("dp_1")
    dims = (((0,), (0,)), ((), ()))
    stores = []
    for k in range(4):
        x = lax.rem(group + k, 4)
        columns = pl.ds(pl.multiple_of((2 * x + me) * wide, wide), wide)
        term = lax.dot_general(
            cotan_ref[:, columns], act_ref[...], dims, preferred_element_type=F32
        ) + lax.dot_general(
            other_cotan_ref[:, columns], other_act_ref[...], dims, preferred_element_type=F32
        )
        sent_ref[k] = term.astype(BF16)
        if k == 0:
            kept_ref[...] = term
            stores.append(pltpu.make_async_copy(kept_ref, kept_hbm, out_sems.at[4]))
            stores[-1].start()
        stores.append(pltpu.make_async_copy(sent_ref.at[k], sent_hbm.at[x], out_sems.at[k]))
        stores[-1].start()
    for store in stores:
        store.wait()


def backward_kernel(
    gain_hbm, shift_hbm, normed_hbm, inv_hbm, halo_hbm, value_hbm, gate_hbm, own_hbm, other_ref,
    cotan_hbm,
    grad_hbm, head_ref, small_ref,
    gain_ref, shift_ref, normed_ref, inv_ref, halo_ref, value_ref, gate_ref, own_ref,
    cotan_ref, grad_ref, gated_ref, cotan_sems, in_sems, out_sem,
):
    length = inv_ref.shape[0]
    blocks = normed_ref.shape[0]
    channels = blocks * LANES
    me = lax.axis_index("dp_1")
    wide = own_ref.shape[1]
    tap_count = 31
    step = 512
    columns = [
        pltpu.make_async_copy(
            cotan_hbm.at[:, pl.ds(pl.multiple_of((2 * x + parity) * wide, wide), wide)],
            cotan_ref.at[4 * n + x],
            cotan_sems.at[4 * n + x],
        )
        for n, parity in enumerate((me, 1 - me))
        for x in range(4)
    ]
    own, *rest = [
        pltpu.make_async_copy(source, target, in_sems.at[n])
        for n, (source, target) in enumerate(
            (
                (own_hbm, own_ref), (gain_hbm, gain_ref),
                (shift_hbm, shift_ref), (normed_hbm, normed_ref), (inv_hbm, inv_ref),
                (halo_hbm, halo_ref), (value_hbm, value_ref), (gate_hbm, gate_ref),
            )
        )
    ]
    for load in (*rest[4:], own, *columns, *rest[:4]):
        load.start()

    def half(n, weight_ref):
        def rows_of(i, carry):
            rows = pl.ds(pl.multiple_of(i * step, step), step)
            total = jnp.dot(cotan_ref[4 * n, rows], weight_ref[0], preferred_element_type=F32)
            for x in range(1, 4):
                total = total + jnp.dot(
                    cotan_ref[4 * n + x, rows], weight_ref[x], preferred_element_type=F32
                )
            for b in range(blocks):
                part = total[:, b * LANES : (b + 1) * LANES]
                grad_ref[b, rows, :] = part + grad_ref[b, rows, :] if n else part
            return carry

        lax.fori_loop(0, length // step, rows_of, 0)

    for load in rest[4:]:
        load.wait()
    for b in range(blocks):
        lanes = slice(b * LANES, (b + 1) * LANES)
        gated_ref[b, 0:HALO, :] = halo_ref[0:HALO, lanes].astype(F32) * sigmoid(
            halo_ref[HALO : 2 * HALO, lanes].astype(F32)
        )

        def gating(i, carry, b=b, lanes=lanes):
            rows = pl.ds(pl.multiple_of(i * 64, 64), 64)
            gated_ref[b, pl.ds(pl.multiple_of(HALO + i * 64, 32), 64), :] = value_ref[
                rows, lanes
            ].astype(F32) * sigmoid(gate_ref[rows, lanes].astype(F32))
            return carry

        lax.fori_loop(0, length // 64, gating, 0)

    for load in (own, *columns[:4]):
        load.wait()
    half(0, own_ref)
    for load in columns[4:]:
        load.wait()
    half(1, other_ref)
    for load in rest[:4]:
        load.wait()

    def point(i, carry):
        rows = pl.ds(pl.multiple_of(i * 128, 128), 128)
        inv = inv_ref[rows, :]
        grads = []
        normeds = []
        gains = []
        shifts = []
        for b in range(blocks):
            lanes = slice(b * LANES, (b + 1) * LANES)
            normed = normed_ref[b, rows, :]
            pre = normed * gain_ref[:, lanes] + shift_ref[:, lanes]
            sig = sigmoid(pre)
            grad_pre = grad_ref[b, rows, :] * (sig + pre * sig * (1.0 - sig))
            gains.append(carry[b] + jnp.sum((grad_pre * normed).reshape(16, 8, LANES), axis=0))
            shifts.append(carry[blocks + b] + jnp.sum(grad_pre.reshape(16, 8, LANES), axis=0))
            grads.append(grad_pre * gain_ref[:, lanes])
            normeds.append(normed)
        first = jnp.sum(sum(grads), axis=-1, keepdims=True) / channels
        second = (
            jnp.sum(sum(g * n for g, n in zip(grads, normeds)), axis=-1, keepdims=True) / channels
        )
        for b in range(blocks):
            grad_ref[b, rows, :] = inv * (grads[b] - first - normeds[b] * second)
        return tuple(gains + shifts)

    zero = jnp.zeros((8, LANES), F32)
    sums = lax.fori_loop(0, length // 128, point, (zero,) * (2 * blocks))
    store = pltpu.make_async_copy(grad_ref, grad_hbm, out_sem)
    store.start()
    for b in range(blocks):
        head_ref[b] = grad_ref[b, 0:HALO, :]
        small_ref[b] = jnp.zeros(small_ref.shape[1:], F32)
        small_ref[b, tap_count : tap_count + 1, :] = jnp.sum(sums[b], axis=0, keepdims=True)
        small_ref[b, tap_count + 1 : tap_count + 2, :] = jnp.sum(
            sums[blocks + b], axis=0, keepdims=True
        )

        def taps(i, carry, b=b):
            start = pl.multiple_of(i * 64, 64)
            grads = [
                grad_ref[b, pl.ds(pl.multiple_of(start + 8 * q, 8), 8), :] for q in range(8)
            ]
            parts = list(carry)
            for o in range(56 + tap_count):
                rows = gated_ref[b, pl.ds(start + (HALO - tap_count + 1 + o), 8), :]
                for q in range(8):
                    if 0 <= o - 8 * q < tap_count:
                        parts[o - 8 * q] = parts[o - 8 * q] + grads[q] * rows
            return tuple(parts)

        parts = lax.fori_loop(0, length // 64, taps, (zero,) * tap_count)
        for j in range(tap_count):
            small_ref[b, j : j + 1, :] = jnp.sum(parts[j], axis=0, keepdims=True)
    store.wait()


def gated_kernel(
    later_ref, taps_ref, grad_hbm, value_hbm, gate_hbm, out_value_ref, out_gate_ref,
    ext_ref, value_ref, gate_ref, sems,
):
    length, channels = value_ref.shape
    blocks = channels // LANES
    tap_count = taps_ref.shape[0]
    loads = []
    for b in range(blocks):
        loads.append(
            pltpu.make_async_copy(grad_hbm.at[b], ext_ref.at[b, pl.ds(0, length)], sems.at[b])
        )
    loads.append(pltpu.make_async_copy(value_hbm, value_ref, sems.at[blocks]))
    loads.append(pltpu.make_async_copy(gate_hbm, gate_ref, sems.at[blocks + 1]))
    for load in loads:
        load.start()
    for b in range(blocks):
        ext_ref[b, length : length + HALO, :] = later_ref[b]
    for load in loads:
        load.wait()
    for b in range(blocks):
        lanes = slice(b * LANES, (b + 1) * LANES)

        def conv(i, carry, b=b, lanes=lanes):
            start = pl.multiple_of(i * 128, 128)
            rows = pl.ds(start, 128)
            totals = convolved(
                lambda o: ext_ref[b, pl.ds(start + o, 8), :],
                [
                    jnp.broadcast_to(taps_ref[j : j + 1, lanes], (8, LANES))
                    for j in reversed(range(tap_count))
                ],
                16,
            )
            total = jnp.concatenate(totals, axis=0)
            sig = sigmoid(gate_ref[rows, lanes].astype(F32))
            part = total * sig
            out_value_ref[rows, lanes] = part.astype(BF16)
            out_gate_ref[rows, lanes] = (
                part * value_ref[rows, lanes].astype(F32) * (1.0 - sig)
            ).astype(BF16)
            return carry

        lax.fori_loop(0, length // 128, conv, 0)


def pack_kernel(parts_ref, kept_ref, small_ref, out_ref):
    count = out_ref.shape[0]
    blocks, small_rows, _ = small_ref.shape
    halves = small_rows // 4
    group = lax.axis_index("dp_0")
    weights = [jnp.where(group == x, 0.0, 1.0) for x in range(4)]
    for i in range(count // 4):
        rows = slice(16 * i, 16 * i + 16)
        tiles = []
        for b in range(blocks):
            lanes = slice(b * LANES, (b + 1) * LANES)
            tiles.append(
                kept_ref[rows, lanes]
                + sum(parts_ref[x, rows, lanes].astype(F32) * weights[x] for x in range(4))
            )
        for k in range(2):
            for h in range(2):
                m = 4 * i + 2 * k + h
                pieces = [tiles[2 * h + t][8 * k : 8 * k + 8] for t in range(2)]
                if m < blocks * halves:
                    b, g = m // halves, m % halves
                    tile = small_ref[b, 4 * g : 4 * g + 4, :]
                    high = tile.astype(BF16).astype(F32)
                    pieces += [high, tile - high]
                else:
                    pieces.append(jnp.zeros((8, LANES), F32))
                out_ref[m] = jnp.concatenate(pieces, axis=0).astype(BF16)


def total_kernel(scale, parts_ref, rows_ref, tiles_ref):
    def add(i, carry):
        return carry + parts_ref[i].astype(F32)

    total = lax.fori_loop(
        0, parts_ref.shape[0], add, jnp.zeros(parts_ref.shape[1:], F32), unroll=8
    ) * scale
    rows_ref[...] = total[0:16]
    tile = jnp.concatenate([total[16:20] + total[20:24], jnp.zeros((4, LANES), F32)], axis=0)
    for i in range(tiles_ref.shape[0]):
        tiles_ref[i] = tile


def spread_kernel(rows_ref, tiles_ref, out_ref):
    tile = sum(tiles_ref[i] for i in range(tiles_ref.shape[0]))[0:4]
    high = tile.astype(BF16).astype(F32)
    both = jnp.concatenate([rows_ref[...], high, tile - high], axis=0).astype(BF16)

    def put(i, carry):
        out_ref[i] = both
        return carry

    lax.fori_loop(0, out_ref.shape[0], put, 0, unroll=8)


def unpack_kernel(parts_ref, weight_ref, taps_ref, gain_ref, shift_ref, small_ref):
    count = parts_ref.shape[0]
    small_rows = small_ref.shape[0]
    tap_count = taps_ref.shape[0]
    blocks = small_ref.shape[1] // LANES
    halves = small_rows // 4
    for m in range(count):
        i, h = m // 2, m % 2
        part = parts_ref[m].astype(F32)
        for t in range(2):
            weight_ref[8 * i : 8 * i + 8, (2 * h + t) * LANES : (2 * h + t + 1) * LANES] = part[
                8 * t : 8 * t + 8
            ]
        if m < blocks * halves:
            b, g = m // halves, m % halves
            small_ref[4 * g : 4 * g + 4, b * LANES : (b + 1) * LANES] = part[16:20] + part[20:24]
    taps_ref[...] = small_ref[0:tap_count, :]
    gain_ref[...] = small_ref[tap_count : tap_count + 1, :]
    shift_ref[...] = small_ref[tap_count + 1 : tap_count + 2, :]


def from_behind(value, axis, by):
    count = lax.axis_size(axis)
    pairs = [(i, i + by) for i in range(count) if 0 <= i + by < count]
    return lax.ppermute(value, axis, pairs)


def swapped(value):
    return lax.ppermute(value, "dp_1", [(0, 1), (1, 0)])


def in_hbm(value):
    return pltpu.with_memory_space_constraint(value, pltpu.HBM)


def exchanged(value, axes):
    return lax.all_to_all(value, axes, 0, 0, tiled=True)


def one_device(glu_value, glu_gate, cotangent, conv_weight, norm_gain, norm_shift, out_weight):
    value_rows = glu_value[0]
    gate_rows = glu_gate[0]
    cotan_rows = cotangent[0]
    length, channels = value_rows.shape
    blocks = channels // LANES
    wide = out_weight.shape[0]
    tap_count = conv_weight.shape[0]
    count_sp = lax.axis_size(SP)
    count_dp = lax.axis_size(DP)
    scale = 1.0 / math.sqrt(length * count_sp * count_dp)
    gain = norm_gain.reshape(1, channels)
    shift = norm_shift.reshape(1, channels)
    shaped = jax.ShapeDtypeStruct

    halo, copies = pl.pallas_call(
        prepare_kernel,
        out_shape=(shaped((2 * HALO, channels), BF16), shaped((4, wide, channels), BF16)),
        in_specs=[HBM] * 3,
        out_specs=(VMEM, HBM),
        scratch_shapes=[pltpu.VMEM((wide, channels), BF16), pltpu.SemaphoreType.DMA((7,))],
        compiler_params=params(62),
        cost_estimate=cost(1),
        name="prepare",
    )(value_rows, gate_rows, out_weight)
    halo = from_behind(halo, SP, 1)
    other_cotan = swapped(cotan_rows)
    own_weight = exchanged(copies, "dp_0")

    act, normed, inv = pl.pallas_call(
        forward_kernel,
        out_shape=(
            shaped((length, channels), BF16),
            pltpu.HBM((blocks, length, LANES), F32),
            pltpu.HBM((length, LANES), F32),
        ),
        in_specs=[VMEM] * 6,
        out_specs=(VMEM, HBM, HBM),
        scratch_shapes=[
            pltpu.VMEM((blocks, length, LANES), F32),
            pltpu.VMEM((length, LANES), F32),
            pltpu.VMEM((blocks, length + HALO, LANES), F32),
            pltpu.SemaphoreType.DMA((2, length // 128)),
        ],
        compiler_params=params(8),
        cost_estimate=cost(6),
        name="module_forward",
    )(conv_weight, gain, shift, halo, value_rows, gate_rows)
    other_act = swapped(act)
    sent, kept = pl.pallas_call(
        weight_kernel,
        out_shape=(pltpu.HBM((4, wide, channels), BF16), pltpu.HBM((wide, channels), F32)),
        in_specs=[VMEM] * 4,
        out_specs=(HBM,) * 2,
        scratch_shapes=[
            pltpu.VMEM((4, wide, channels), BF16),
            pltpu.VMEM((wide, channels), F32),
            pltpu.SemaphoreType.DMA((5,)),
        ],
        compiler_params=params(8),
        cost_estimate=cost(3),
        name="weight_term",
    )(act, other_act, cotan_rows, other_cotan)
    own_weight, kept = lax.optimization_barrier((own_weight, kept))
    other_weight = swapped(own_weight)
    arrived = exchanged(sent, "dp_0")

    small_rows = -(-(tap_count + 2) // 8) * 8
    grad, head, small = pl.pallas_call(
        backward_kernel,
        out_shape=(
            pltpu.HBM((blocks, length, LANES), F32),
            shaped((blocks, HALO, LANES), F32),
            shaped((blocks, small_rows, LANES), F32),
        ),
        in_specs=[HBM] * 8 + [VMEM, HBM],
        out_specs=(HBM, VMEM, VMEM),
        scratch_shapes=[
            pltpu.VMEM((1, channels), F32),
            pltpu.VMEM((1, channels), F32),
            pltpu.VMEM((blocks, length, LANES), F32),
            pltpu.VMEM((length, LANES), F32),
            pltpu.VMEM((2 * HALO, channels), BF16),
            pltpu.VMEM((length, channels), BF16),
            pltpu.VMEM((length, channels), BF16),
            pltpu.VMEM((4, wide, channels), BF16),
            pltpu.VMEM((8, length, wide), BF16),
            pltpu.VMEM((blocks, length, LANES), F32),
            pltpu.VMEM((blocks, length + HALO, LANES), F32),
            pltpu.SemaphoreType.DMA((8,)),
            pltpu.SemaphoreType.DMA((8,)),
            pltpu.SemaphoreType.DMA,
        ],
        compiler_params=params(14),
        cost_estimate=cost(10),
        name="module_backward",
    )(
        *(in_hbm(a) for a in (gain, shift, normed, inv, halo, value_rows, gate_rows)),
        in_hbm(own_weight), other_weight, in_hbm(cotan_rows),
    )
    later = from_behind(head, SP, -1)

    packed = pl.pallas_call(
        pack_kernel,
        out_shape=shaped((count_sp, 24, LANES), BF16),
        in_specs=[VMEM] * 3,
        out_specs=VMEM,
        compiler_params=params(8),
        cost_estimate=cost(1),
        name="pack",
    )(arrived, kept, small)
    grad_value, grad_gate = pl.pallas_call(
        gated_kernel,
        out_shape=(shaped((length, channels), BF16), shaped((length, channels), BF16)),
        in_specs=[VMEM] * 2 + [HBM] * 3,
        out_specs=(VMEM,) * 2,
        scratch_shapes=[
            pltpu.VMEM((blocks, length + HALO, LANES), F32),
            pltpu.VMEM((length, channels), BF16),
            pltpu.VMEM((length, channels), BF16),
            pltpu.SemaphoreType.DMA((blocks + 2,)),
        ],
        compiler_params=params(62),
        cost_estimate=cost(6),
        name="gated_backward",
    )(later, conv_weight, grad, value_rows, gate_rows)

    terms = exchanged(packed, SP)
    rows, tiles = pl.pallas_call(
        functools.partial(total_kernel, scale),
        out_shape=(shaped((16, LANES), F32), shaped((count_dp, 8, LANES), F32)),
        in_specs=[VMEM],
        out_specs=(VMEM,) * 2,
        compiler_params=params(4),
        cost_estimate=cost(1),
        name="total",
    )(terms)
    tiles = exchanged(tiles, DP)
    totals = pl.pallas_call(
        spread_kernel,
        out_shape=shaped((count_sp, 24, LANES), BF16),
        in_specs=[VMEM] * 2,
        out_specs=VMEM,
        compiler_params=params(4),
        cost_estimate=cost(1),
        name="spread",
    )(rows, tiles)
    whole = exchanged(totals, SP)
    grad_out_weight, grad_conv, grad_gain, grad_shift = pl.pallas_call(
        unpack_kernel,
        out_shape=(
            shaped((wide, channels), F32),
            shaped((tap_count, channels), F32),
            shaped((1, channels), F32),
            shaped((1, channels), F32),
        ),
        in_specs=[VMEM],
        out_specs=(VMEM,) * 4,
        scratch_shapes=[pltpu.VMEM((small_rows, channels), F32)],
        compiler_params=params(8),
        cost_estimate=cost(1),
        name="unpack",
    )(whole)
    return (
        grad_value[None],
        grad_gate[None],
        grad_out_weight,
        grad_conv,
        grad_gain.reshape(channels),
        grad_shift.reshape(channels),
    )


def solution(mesh):
    split = Mesh(mesh.devices.reshape(8, 8, 4, 2), ("sp_0", "sp_1", "dp_0", "dp_1"))
    return jax.shard_map(
        one_device,
        mesh=split,
        in_specs=(P(DP, SP, None), P(DP, SP, None), P(DP, SP, None), P(), P(), P(), P(DP, None)),
        out_specs=(P(DP, SP, None), P(DP, SP, None), P(DP, None), P(), P(), P()),
        check_vma=False,
    )
```

```python
import functools
import math

import jax
import jax.numpy as jnp
from jax import lax
from jax.experimental import pallas as pl
from jax.experimental.pallas import tpu as pltpu
from jax.sharding import Mesh
from jax.sharding import PartitionSpec as P


SP = ("sp_0", "sp_1")
DP = ("dp_0", "dp_1")

epsilon = 1e-06

LANES = 128
HALO = 32
BF16 = jnp.bfloat16
F32 = jnp.float32
VMEM = pl.BlockSpec(memory_space=pltpu.VMEM)
HBM = pl.BlockSpec(memory_space=pltpu.HBM)


def params(mib=16):
    return pltpu.CompilerParams(vmem_limit_bytes=mib * 1024 * 1024)


def cost(us):
    return pl.CostEstimate(flops=int(us * 5.0e8), bytes_accessed=1 << 20, transcendentals=0)


def sigmoid(x):
    return 0.5 * jnp.tanh(0.5 * x) + 0.5


def convolved(load, weights, groups):
    totals = [None] * groups
    for o in range(8 * (groups - 1) + len(weights)):
        rows = load(o)
        for q in range(groups):
            j = o - 8 * q
            if 0 <= j < len(weights):
                term = weights[j] * rows
                totals[q] = term if totals[q] is None else totals[q] + term
    return totals


def prepare_kernel(value_hbm, gate_hbm, weight_hbm, halo_ref, copies_hbm, weight_ref, sems):
    length = value_hbm.shape[0]
    tail = pl.ds(length - HALO, HALO)
    loads = [
        pltpu.make_async_copy(weight_hbm, weight_ref, sems.at[0]),
        pltpu.make_async_copy(value_hbm.at[tail], halo_ref.at[pl.ds(0, HALO)], sems.at[1]),
        pltpu.make_async_copy(gate_hbm.at[tail], halo_ref.at[pl.ds(HALO, HALO)], sems.at[2]),
    ]
    for load in loads:
        load.start()
    loads[0].wait()
    stores = [
        pltpu.make_async_copy(weight_ref, copies_hbm.at[x], sems.at[3 + x]) for x in range(4)
    ]
    for store in stores:
        store.start()
    for copy in loads[1:] + stores:
        copy.wait()


def forward_kernel(
    taps_ref, gain_ref, shift_ref, halo_ref, value_ref, gate_ref,
    act_ref, normed_hbm, inv_hbm,
    normed_ref, inv_ref, gated_ref, out_sems,
):
    length, channels = value_ref.shape
    blocks = channels // LANES
    tap_count = taps_ref.shape[0]
    step = 128
    steps = length // step

    def row_stores(i):
        rows = pl.ds(pl.multiple_of(i * step, step), step)
        return [
            pltpu.make_async_copy(inv_ref.at[rows], inv_hbm.at[rows], out_sems.at[0, i]),
            pltpu.make_async_copy(
                normed_ref.at[:, rows], normed_hbm.at[:, rows], out_sems.at[1, i]
            ),
        ]

    for b in range(blocks):
        lanes = slice(b * LANES, (b + 1) * LANES)
        gated_ref[b, 0:HALO, :] = halo_ref[0:HALO, lanes].astype(F32) * sigmoid(
            halo_ref[HALO : 2 * HALO, lanes].astype(F32)
        )

    def group(i, carry):
        start = pl.multiple_of(i * step, step)
        rows = pl.ds(start, step)
        for b in range(blocks):
            lanes = slice(b * LANES, (b + 1) * LANES)
            gated_ref[b, pl.ds(pl.multiple_of(HALO + start, 32), step), :] = value_ref[
                rows, lanes
            ].astype(F32) * sigmoid(gate_ref[rows, lanes].astype(F32))
        for b in range(blocks):
            lanes = slice(b * LANES, (b + 1) * LANES)
            totals = convolved(
                lambda o: gated_ref[b, pl.ds(start + (HALO - tap_count + 1 + o), 8), :],
                [
                    jnp.broadcast_to(taps_ref[j : j + 1, lanes], (8, LANES))
                    for j in range(tap_count)
                ],
                step // 8,
            )
            for q, total in enumerate(totals):
                normed_ref[b, pl.ds(pl.multiple_of(start + 8 * q, 8), 8), :] = total
        parts = [normed_ref[b, rows, :] for b in range(blocks)]
        mean = jnp.sum(sum(parts), axis=-1, keepdims=True) / channels
        centred = [p - mean for p in parts]
        var = jnp.sum(sum(p * p for p in centred), axis=-1, keepdims=True) / channels
        inv = lax.rsqrt(var + epsilon)
        inv_ref[rows, :] = jnp.broadcast_to(inv, (step, LANES))
        for b in range(blocks):
            lanes = slice(b * LANES, (b + 1) * LANES)
            normed = centred[b] * inv
            normed_ref[b, rows, :] = normed
            pre = normed * gain_ref[:, lanes] + shift_ref[:, lanes]
            act_ref[rows, lanes] = (pre * sigmoid(pre)).astype(BF16)
        for store in row_stores(i):
            store.start()
        return carry

    lax.fori_loop(0, steps, group, 0)
    for i in range(steps):
        for store in row_stores(i):
            store.wait()


def weight_kernel(
    act_ref, other_act_ref, cotan_ref, other_cotan_ref, sent_hbm, kept_hbm,
    sent_ref, kept_ref, out_sems,
):
    wide = sent_ref.shape[1]
    group, me = lax.axis_index("dp_0"), lax.axis_index("dp_1")
    dims = (((0,), (0,)), ((), ()))
    stores = []
    for k in range(4):
        x = lax.rem(group + k, 4)
        columns = pl.ds(pl.multiple_of((2 * x + me) * wide, wide), wide)
        term = lax.dot_general(
            cotan_ref[:, columns], act_ref[...], dims, preferred_element_type=F32
        ) + lax.dot_general(
            other_cotan_ref[:, columns], other_act_ref[...], dims, preferred_element_type=F32
        )
        sent_ref[k] = term.astype(BF16)
        if k == 0:
            kept_ref[...] = term
            stores.append(pltpu.make_async_copy(kept_ref, kept_hbm, out_sems.at[4]))
            stores[-1].start()
        stores.append(pltpu.make_async_copy(sent_ref.at[k], sent_hbm.at[x], out_sems.at[k]))
        stores[-1].start()
    for store in stores:
        store.wait()


def backward_kernel(
    gain_hbm, shift_hbm, normed_hbm, inv_hbm, halo_hbm, value_hbm, gate_hbm, own_hbm, other_ref,
    cotan_hbm,
    grad_hbm, head_ref, small_ref,
    gain_ref, shift_ref, normed_ref, inv_ref, halo_ref, value_ref, gate_ref, own_ref,
    cotan_ref, grad_ref, gated_ref, cotan_sems, in_sems, out_sem,
):
    length = inv_ref.shape[0]
    blocks = normed_ref.shape[0]
    channels = blocks * LANES
    me = lax.axis_index("dp_1")
    wide = own_ref.shape[1]
    tap_count = 31
    step = 512
    columns = [
        pltpu.make_async_copy(
            cotan_hbm.at[:, pl.ds(pl.multiple_of((2 * x + parity) * wide, wide), wide)],
            cotan_ref.at[4 * n + x],
            cotan_sems.at[4 * n + x],
        )
        for n, parity in enumerate((me, 1 - me))
        for x in range(4)
    ]
    own, *rest = [
        pltpu.make_async_copy(source, target, in_sems.at[n])
        for n, (source, target) in enumerate(
            (
                (own_hbm, own_ref), (gain_hbm, gain_ref),
                (shift_hbm, shift_ref), (normed_hbm, normed_ref), (inv_hbm, inv_ref),
                (halo_hbm, halo_ref), (value_hbm, value_ref), (gate_hbm, gate_ref),
            )
        )
    ]
    for load in (*rest[4:], own, *columns, *rest[:4]):
        load.start()

    def half(n, weight_ref):
        def rows_of(i, carry):
            rows = pl.ds(pl.multiple_of(i * step, step), step)
            total = jnp.dot(cotan_ref[4 * n, rows], weight_ref[0], preferred_element_type=F32)
            for x in range(1, 4):
                total = total + jnp.dot(
                    cotan_ref[4 * n + x, rows], weight_ref[x], preferred_element_type=F32
                )
            for b in range(blocks):
                part = total[:, b * LANES : (b + 1) * LANES]
                grad_ref[b, rows, :] = part + grad_ref[b, rows, :] if n else part
            return carry

        lax.fori_loop(0, length // step, rows_of, 0)

    for load in rest[4:]:
        load.wait()
    for b in range(blocks):
        lanes = slice(b * LANES, (b + 1) * LANES)
        gated_ref[b, 0:HALO, :] = halo_ref[0:HALO, lanes].astype(F32) * sigmoid(
            halo_ref[HALO : 2 * HALO, lanes].astype(F32)
        )

        def gating(i, carry, b=b, lanes=lanes):
            rows = pl.ds(pl.multiple_of(i * 64, 64), 64)
            gated_ref[b, pl.ds(pl.multiple_of(HALO + i * 64, 32), 64), :] = value_ref[
                rows, lanes
            ].astype(F32) * sigmoid(gate_ref[rows, lanes].astype(F32))
            return carry

        lax.fori_loop(0, length // 64, gating, 0)

    for load in (own, *columns[:4]):
        load.wait()
    half(0, own_ref)
    for load in columns[4:]:
        load.wait()
    half(1, other_ref)
    for load in rest[:4]:
        load.wait()

    def point(i, carry):
        rows = pl.ds(pl.multiple_of(i * 128, 128), 128)
        inv = inv_ref[rows, :]
        grads = []
        normeds = []
        gains = []
        shifts = []
        for b in range(blocks):
            lanes = slice(b * LANES, (b + 1) * LANES)
            normed = normed_ref[b, rows, :]
            pre = normed * gain_ref[:, lanes] + shift_ref[:, lanes]
            sig = sigmoid(pre)
            grad_pre = grad_ref[b, rows, :] * (sig + pre * sig * (1.0 - sig))
            gains.append(carry[b] + jnp.sum((grad_pre * normed).reshape(16, 8, LANES), axis=0))
            shifts.append(carry[blocks + b] + jnp.sum(grad_pre.reshape(16, 8, LANES), axis=0))
            grads.append(grad_pre * gain_ref[:, lanes])
            normeds.append(normed)
        first = jnp.sum(sum(grads), axis=-1, keepdims=True) / channels
        second = (
            jnp.sum(sum(g * n for g, n in zip(grads, normeds)), axis=-1, keepdims=True) / channels
        )
        for b in range(blocks):
            grad_ref[b, rows, :] = inv * (grads[b] - first - normeds[b] * second)
        return tuple(gains + shifts)

    zero = jnp.zeros((8, LANES), F32)
    sums = lax.fori_loop(0, length // 128, point, (zero,) * (2 * blocks))
    store = pltpu.make_async_copy(grad_ref, grad_hbm, out_sem)
    store.start()
    for b in range(blocks):
        head_ref[b] = grad_ref[b, 0:HALO, :]
        small_ref[b] = jnp.zeros(small_ref.shape[1:], F32)
        small_ref[b, tap_count : tap_count + 1, :] = jnp.sum(sums[b], axis=0, keepdims=True)
        small_ref[b, tap_count + 1 : tap_count + 2, :] = jnp.sum(
            sums[blocks + b], axis=0, keepdims=True
        )

        def taps(i, carry, b=b):
            start = pl.multiple_of(i * 64, 64)
            grads = [
                grad_ref[b, pl.ds(pl.multiple_of(start + 8 * q, 8), 8), :] for q in range(8)
            ]
            parts = list(carry)
            for o in range(56 + tap_count):
                rows = gated_ref[b, pl.ds(start + (HALO - tap_count + 1 + o), 8), :]
                for q in range(8):
                    if 0 <= o - 8 * q < tap_count:
                        parts[o - 8 * q] = parts[o - 8 * q] + grads[q] * rows
            return tuple(parts)

        parts = lax.fori_loop(0, length // 64, taps, (zero,) * tap_count)
        for j in range(tap_count):
            small_ref[b, j : j + 1, :] = jnp.sum(parts[j], axis=0, keepdims=True)
    store.wait()


def gated_kernel(
    later_ref, taps_ref, grad_hbm, value_hbm, gate_hbm, out_value_ref, out_gate_ref,
    ext_ref, value_ref, gate_ref, sems,
):
    length, channels = value_ref.shape
    blocks = channels // LANES
    tap_count = taps_ref.shape[0]
    loads = []
    for b in range(blocks):
        loads.append(
            pltpu.make_async_copy(grad_hbm.at[b], ext_ref.at[b, pl.ds(0, length)], sems.at[b])
        )
    loads.append(pltpu.make_async_copy(value_hbm, value_ref, sems.at[blocks]))
    loads.append(pltpu.make_async_copy(gate_hbm, gate_ref, sems.at[blocks + 1]))
    for load in loads:
        load.start()
    for b in range(blocks):
        ext_ref[b, length : length + HALO, :] = later_ref[b]
    for load in loads:
        load.wait()
    for b in range(blocks):
        lanes = slice(b * LANES, (b + 1) * LANES)

        def conv(i, carry, b=b, lanes=lanes):
            start = pl.multiple_of(i * 128, 128)
            rows = pl.ds(start, 128)
            totals = convolved(
                lambda o: ext_ref[b, pl.ds(start + o, 8), :],
                [
                    jnp.broadcast_to(taps_ref[j : j + 1, lanes], (8, LANES))
                    for j in reversed(range(tap_count))
                ],
                16,
            )
            total = jnp.concatenate(totals, axis=0)
            sig = sigmoid(gate_ref[rows, lanes].astype(F32))
            part = total * sig
            out_value_ref[rows, lanes] = part.astype(BF16)
            out_gate_ref[rows, lanes] = (
                part * value_ref[rows, lanes].astype(F32) * (1.0 - sig)
            ).astype(BF16)
            return carry

        lax.fori_loop(0, length // 128, conv, 0)


def pack_kernel(parts_ref, kept_ref, small_ref, out_ref):
    count = out_ref.shape[0]
    blocks, small_rows, _ = small_ref.shape
    halves = small_rows // 4
    group = lax.axis_index("dp_0")
    weights = [jnp.where(group == x, 0.0, 1.0) for x in range(4)]
    for i in range(count // 4):
        rows = slice(16 * i, 16 * i + 16)
        tiles = []
        for b in range(blocks):
            lanes = slice(b * LANES, (b + 1) * LANES)
            tiles.append(
                kept_ref[rows, lanes]
                + sum(parts_ref[x, rows, lanes].astype(F32) * weights[x] for x in range(4))
            )
        for k in range(2):
            for h in range(2):
                m = 4 * i + 2 * k + h
                pieces = [tiles[2 * h + t][8 * k : 8 * k + 8] for t in range(2)]
                if m < blocks * halves:
                    b, g = m // halves, m % halves
                    tile = small_ref[b, 4 * g : 4 * g + 4, :]
                    high = tile.astype(BF16).astype(F32)
                    pieces += [high, tile - high]
                else:
                    pieces.append(jnp.zeros((8, LANES), F32))
                out_ref[m] = jnp.concatenate(pieces, axis=0).astype(BF16)


def total_kernel(scale, parts_ref, rows_ref, tiles_ref):
    def add(i, carry):
        return carry + parts_ref[i].astype(F32)

    total = lax.fori_loop(
        0, parts_ref.shape[0], add, jnp.zeros(parts_ref.shape[1:], F32), unroll=8
    ) * scale
    rows_ref[...] = total[0:16]
    tile = total[16:20] + total[20:24]
    for i in range(tiles_ref.shape[0]):
        tiles_ref[i] = tile


def spread_kernel(rows_ref, tiles_ref, out_ref):
    tile = sum(tiles_ref[i] for i in range(tiles_ref.shape[0]))
    high = tile.astype(BF16).astype(F32)
    both = jnp.concatenate([rows_ref[...], high, tile - high], axis=0).astype(BF16)

    def put(i, carry):
        out_ref[i] = both
        return carry

    lax.fori_loop(0, out_ref.shape[0], put, 0, unroll=8)


def unpack_kernel(
    parts_ref, weight_hbm, taps_ref, gain_ref, shift_ref, small_ref, weight_ref, sems
):
    count = parts_ref.shape[0]
    small_rows = small_ref.shape[0]
    tap_count = taps_ref.shape[0]
    blocks = small_ref.shape[1] // LANES
    halves = small_rows // 4
    rows = weight_ref.shape[0] // 4
    stores = []
    for m in range(count):
        i, h = m // 2, m % 2
        part = parts_ref[m].astype(F32)
        for t in range(2):
            weight_ref[8 * i : 8 * i + 8, (2 * h + t) * LANES : (2 * h + t + 1) * LANES] = part[
                8 * t : 8 * t + 8
            ]
        if m < blocks * halves:
            b, g = m // halves, m % halves
            small_ref[4 * g : 4 * g + 4, b * LANES : (b + 1) * LANES] = part[16:20] + part[20:24]
        if (m + 1) % (count // 4) == 0:
            n = m // (count // 4)
            span = pl.ds(n * rows, rows)
            stores.append(
                pltpu.make_async_copy(weight_ref.at[span], weight_hbm.at[span], sems.at[n])
            )
            stores[-1].start()
    taps_ref[...] = small_ref[0:tap_count, :]
    gain_ref[...] = small_ref[tap_count : tap_count + 1, :]
    shift_ref[...] = small_ref[tap_count + 1 : tap_count + 2, :]
    for store in stores:
        store.wait()


def from_behind(value, axis, by):
    count = lax.axis_size(axis)
    pairs = [(i, i + by) for i in range(count) if 0 <= i + by < count]
    return lax.ppermute(value, axis, pairs)


def swapped(value):
    return lax.ppermute(value, "dp_1", [(0, 1), (1, 0)])


def in_hbm(value):
    return pltpu.with_memory_space_constraint(value, pltpu.HBM)


def exchanged(value, axes):
    return lax.all_to_all(value, axes, 0, 0, tiled=True)


def one_device(glu_value, glu_gate, cotangent, conv_weight, norm_gain, norm_shift, out_weight):
    value_rows = glu_value[0]
    gate_rows = glu_gate[0]
    cotan_rows = cotangent[0]
    length, channels = value_rows.shape
    blocks = channels // LANES
    wide = out_weight.shape[0]
    tap_count = conv_weight.shape[0]
    count_sp = lax.axis_size(SP)
    count_dp = lax.axis_size(DP)
    scale = 1.0 / math.sqrt(length * count_sp * count_dp)
    gain = norm_gain.reshape(1, channels)
    shift = norm_shift.reshape(1, channels)
    shaped = jax.ShapeDtypeStruct

    halo, copies = pl.pallas_call(
        prepare_kernel,
        out_shape=(shaped((2 * HALO, channels), BF16), shaped((4, wide, channels), BF16)),
        in_specs=[HBM] * 3,
        out_specs=(VMEM, HBM),
        scratch_shapes=[pltpu.VMEM((wide, channels), BF16), pltpu.SemaphoreType.DMA((7,))],
        compiler_params=params(62),
        cost_estimate=cost(1),
        name="prepare",
    )(value_rows, gate_rows, out_weight)
    halo = from_behind(halo, SP, 1)
    other_cotan = swapped(cotan_rows)
    own_weight = exchanged(copies, "dp_0")

    act, normed, inv = pl.pallas_call(
        forward_kernel,
        out_shape=(
            shaped((length, channels), BF16),
            pltpu.HBM((blocks, length, LANES), F32),
            pltpu.HBM((length, LANES), F32),
        ),
        in_specs=[VMEM] * 6,
        out_specs=(VMEM, HBM, HBM),
        scratch_shapes=[
            pltpu.VMEM((blocks, length, LANES), F32),
            pltpu.VMEM((length, LANES), F32),
            pltpu.VMEM((blocks, length + HALO, LANES), F32),
            pltpu.SemaphoreType.DMA((2, length // 128)),
        ],
        compiler_params=params(8),
        cost_estimate=cost(6),
        name="module_forward",
    )(conv_weight, gain, shift, halo, value_rows, gate_rows)
    other_act = swapped(act)
    sent, kept = pl.pallas_call(
        weight_kernel,
        out_shape=(pltpu.HBM((4, wide, channels), BF16), pltpu.HBM((wide, channels), F32)),
        in_specs=[VMEM] * 4,
        out_specs=(HBM,) * 2,
        scratch_shapes=[
            pltpu.VMEM((4, wide, channels), BF16),
            pltpu.VMEM((wide, channels), F32),
            pltpu.SemaphoreType.DMA((5,)),
        ],
        compiler_params=params(8),
        cost_estimate=cost(3),
        name="weight_term",
    )(act, other_act, cotan_rows, other_cotan)
    own_weight, kept = lax.optimization_barrier((own_weight, kept))
    other_weight = swapped(own_weight)
    arrived = exchanged(sent, "dp_0")

    small_rows = -(-(tap_count + 2) // 8) * 8
    grad, head, small = pl.pallas_call(
        backward_kernel,
        out_shape=(
            pltpu.HBM((blocks, length, LANES), F32),
            shaped((blocks, HALO, LANES), F32),
            shaped((blocks, small_rows, LANES), F32),
        ),
        in_specs=[HBM] * 8 + [VMEM, HBM],
        out_specs=(HBM, VMEM, VMEM),
        scratch_shapes=[
            pltpu.VMEM((1, channels), F32),
            pltpu.VMEM((1, channels), F32),
            pltpu.VMEM((blocks, length, LANES), F32),
            pltpu.VMEM((length, LANES), F32),
            pltpu.VMEM((2 * HALO, channels), BF16),
            pltpu.VMEM((length, channels), BF16),
            pltpu.VMEM((length, channels), BF16),
            pltpu.VMEM((4, wide, channels), BF16),
            pltpu.VMEM((8, length, wide), BF16),
            pltpu.VMEM((blocks, length, LANES), F32),
            pltpu.VMEM((blocks, length + HALO, LANES), F32),
            pltpu.SemaphoreType.DMA((8,)),
            pltpu.SemaphoreType.DMA((8,)),
            pltpu.SemaphoreType.DMA,
        ],
        compiler_params=params(14),
        cost_estimate=cost(10),
        name="module_backward",
    )(
        *(in_hbm(a) for a in (gain, shift, normed, inv, halo, value_rows, gate_rows)),
        in_hbm(own_weight), other_weight, in_hbm(cotan_rows),
    )
    later = from_behind(head, SP, -1)

    packed = pl.pallas_call(
        pack_kernel,
        out_shape=shaped((count_sp, 24, LANES), BF16),
        in_specs=[VMEM] * 3,
        out_specs=VMEM,
        compiler_params=params(8),
        cost_estimate=cost(1),
        name="pack",
    )(arrived, kept, small)
    grad_value, grad_gate = pl.pallas_call(
        gated_kernel,
        out_shape=(shaped((length, channels), BF16), shaped((length, channels), BF16)),
        in_specs=[VMEM] * 2 + [HBM] * 3,
        out_specs=(VMEM,) * 2,
        scratch_shapes=[
            pltpu.VMEM((blocks, length + HALO, LANES), F32),
            pltpu.VMEM((length, channels), BF16),
            pltpu.VMEM((length, channels), BF16),
            pltpu.SemaphoreType.DMA((blocks + 2,)),
        ],
        compiler_params=params(62),
        cost_estimate=cost(6),
        name="gated_backward",
    )(later, conv_weight, grad, value_rows, gate_rows)

    terms = exchanged(packed, SP)
    rows, tiles = pl.pallas_call(
        functools.partial(total_kernel, scale),
        out_shape=(shaped((16, LANES), F32), shaped((count_dp, 4, LANES), F32)),
        in_specs=[VMEM],
        out_specs=(VMEM,) * 2,
        compiler_params=params(4),
        cost_estimate=cost(1),
        name="total",
    )(terms)
    tiles = exchanged(tiles, DP)
    totals = pl.pallas_call(
        spread_kernel,
        out_shape=shaped((count_sp, 24, LANES), BF16),
        in_specs=[VMEM] * 2,
        out_specs=VMEM,
        compiler_params=params(4),
        cost_estimate=cost(1),
        name="spread",
    )(rows, tiles)
    whole = exchanged(totals, SP)
    grad_out_weight, grad_conv, grad_gain, grad_shift = pl.pallas_call(
        unpack_kernel,
        out_shape=(
            shaped((wide, channels), F32),
            shaped((tap_count, channels), F32),
            shaped((1, channels), F32),
            shaped((1, channels), F32),
        ),
        in_specs=[VMEM],
        out_specs=(HBM,) + (VMEM,) * 3,
        scratch_shapes=[
            pltpu.VMEM((small_rows, channels), F32),
            pltpu.VMEM((wide, channels), F32),
            pltpu.SemaphoreType.DMA((4,)),
        ],
        compiler_params=params(8),
        cost_estimate=cost(1),
        name="unpack",
    )(whole)
    return (
        grad_value[None],
        grad_gate[None],
        grad_out_weight,
        grad_conv,
        grad_gain.reshape(channels),
        grad_shift.reshape(channels),
    )


def solution(mesh):
    split = Mesh(mesh.devices.reshape(8, 8, 4, 2), ("sp_0", "sp_1", "dp_0", "dp_1"))
    return jax.shard_map(
        one_device,
        mesh=split,
        in_specs=(P(DP, SP, None), P(DP, SP, None), P(DP, SP, None), P(), P(), P(), P(DP, None)),
        out_specs=(P(DP, SP, None), P(DP, SP, None), P(DP, None), P(), P(), P()),
        check_vma=False,
    )
```
